32 devices in a mesh: sp: 8 (over z, y), tp: 4 (over x, core).
Axes of the slice: x: 2, y: 2, z: 4, core: 2. Of those that a mesh axis runs over, the one named last changes fastest.
Arguments:
- tokens: bfloat16 [3072, 2048], P('sp', 'tp'), may hold values from -6 to 6
- norm_gain: float32 [2048], replicated, may hold values from 0.1 to 1.9
- w_query_down: bfloat16 [2048, 512], replicated, may hold values from -0.125 to 0.125
- query_gain: float32 [512], replicated, may hold values from 0.1 to 1.9
- w_query_up: bfloat16 [512, 1536], P(None, 'tp'), may hold values from -0.25 to 0.25
- w_latent_down: bfloat16 [2048, 256], replicated, may hold values from -0.125 to 0.125
- latent_gain: float32 [256], replicated, may hold values from 0.1 to 1.9
- w_rotary_key: bfloat16 [2048, 32], replicated, may hold values from -0.125 to 0.125
- w_latent_up: bfloat16 [256, 2048], P(None, 'tp'), may hold values from -0.375 to 0.375
- query_head_gain: float32 [96], replicated, may hold values from 0.1 to 1.9
- key_head_gain: float32 [96], replicated, may hold values from 0.1 to 1.9
- w_pool_in: bfloat16 [2048, 1024], P(None, 'tp'), may hold values from -0.125 to 0.125
- w_pool_mix: bfloat16 [4, 256, 256], P('tp'), may hold values from -0.375 to 0.375
- pool_scale: float32 [1024], P('tp'), may hold values from 0.1 to 1.9
- w_attn_out: bfloat16 [1024, 2048], P('tp'), may hold values from -12 to 12
- w_pool_out: bfloat16 [1024, 2048], P('tp'), may hold values from -0.5 to 0.5
- w_gate_attn: bfloat16 [2048, 2048], P(None, 'tp'), may hold values from -0.125 to 0.125
- w_gate_pool: bfloat16 [2048, 2048], P(None, 'tp'), may hold values from -0.125 to 0.125
Outputs:
- mixed: bfloat16 [3072, 2048], P('sp', 'tp')
The draws below stay inside these ranges and needn't reach their ends.
All inputs are finite; a program needn't handle non-finite values.
Results may differ from the reference program's by a relative error of at most 0.02.
Values may be sent and summed in bfloat16 or wider, within the bound.
A program may use at most 128 MiB of HBM per device.

```python
import math
import jax
import jax.numpy as jnp
from jax import lax

D = 2048
HEADS = 16
QUERY_RANK = 512
LATENT_RANK = 256
NOPE = 64
ROPE = 32
VALUE_DIM = 64
POOL_GROUPS = 4
POOL_GROUP = 256
POOL_WIDTH = 1024
TOKENS = 3072


def level_of(rng, extent, pieces, smallest, top_value):
    def one(dim, shards_of):
        steps = jax.random.uniform(jax.random.fold_in(jax.random.fold_in(rng, 6), dim), (shards_of,), jnp.float32, smallest / len(pieces), top_value / len(pieces))
        return jnp.repeat(jnp.exp(steps), extent[dim] // shards_of).reshape((-1,) + (1,) * (len(extent) - dim - 1))

    level = one(*pieces[0])
    for cut in pieces[1:]:
        level = level * one(*cut)
    return level


def centred(own_key, shape, deviation, most, split=(), held_as=jnp.bfloat16):
    result = jax.random.normal(own_key, shape, jnp.float32) * deviation
    if len(split) > 0:
        result = level_of(own_key, shape, split, -0.22, 0.18) * result
    return jnp.clip(result, min=-most, max=most).astype(held_as)


def setup_inputs(seed: int = 0) -> dict:
    streams_of = jax.random.split(jax.random.key(seed), 19)
    return {
        "tokens": centred(streams_of[0], (TOKENS, D), 1.0, 6.0, ((0, 8), (1, 4))),
        "norm_gain": jnp.clip(1.0 + 0.18 * jax.random.normal(streams_of[1], (D,), jnp.float32), 0.1, 1.9),
        "w_query_down": centred(streams_of[2], (D, QUERY_RANK), D ** -0.5, 0.125),
        "query_gain": jnp.clip(1.0 + 0.18 * jax.random.normal(streams_of[3], (QUERY_RANK,), jnp.float32), 0.1, 1.9),
        "w_query_up": centred(streams_of[4], (QUERY_RANK, HEADS * (NOPE + ROPE)), QUERY_RANK ** -0.5, 0.25, ((1, 4),)),
        "w_latent_down": centred(streams_of[5], (D, LATENT_RANK), D ** -0.5, 0.125),
        "latent_gain": jnp.clip(1.0 + 0.18 * jax.random.normal(streams_of[6], (LATENT_RANK,), jnp.float32), 0.1, 1.9),
        "w_rotary_key": centred(streams_of[7], (D, ROPE), D ** -0.5, 0.125),
        "w_latent_up": centred(streams_of[8], (LATENT_RANK, HEADS * (NOPE + VALUE_DIM)), LATENT_RANK ** -0.5, 0.375, ((1, 4),)),
        "query_head_gain": jnp.clip(1.0 + 0.18 * jax.random.normal(streams_of[9], (NOPE + ROPE,), jnp.float32), 0.1, 1.9),
        "key_head_gain": jnp.clip(1.0 + 0.18 * jax.random.normal(streams_of[10], (NOPE + ROPE,), jnp.float32), 0.1, 1.9),
        "w_pool_in": centred(streams_of[11], (D, POOL_WIDTH), D ** -0.5, 0.125, ((1, 4),)),
        "w_pool_mix": centred(streams_of[12], (POOL_GROUPS, POOL_GROUP, POOL_GROUP), POOL_GROUP ** -0.5, 0.375, ((0, 4),)),
        "pool_scale": jnp.clip(1.0 + 0.18 * jax.random.normal(streams_of[13], (POOL_WIDTH,), jnp.float32), 0.1, 1.9),
        "w_attn_out": centred(streams_of[14], (HEADS * VALUE_DIM, D), 2.0, 12.0, ((0, 4),)),
        "w_pool_out": centred(streams_of[15], (POOL_WIDTH, D), (POOL_WIDTH // 8) ** -0.5, 0.5, ((0, 4),)),
        "w_gate_attn": centred(streams_of[16], (D, D), D ** -0.5, 0.125, ((1, 4),)),
        "w_gate_pool": centred(streams_of[17], (D, D), D ** -0.5, 0.125, ((1, 4),)),
    }


eps = 1e-06
theta = 10000.0

def rms_scale(values, gain):
    values = values.astype(jnp.float32)
    return values * lax.rsqrt(lax.optimization_barrier(jnp.mean(values * values, axis=-1, keepdims=True)) + eps) * gain

def rotate(values, positions):
    half = values.shape[-1] // 2
    freqs = theta ** (-jnp.arange(half, dtype=jnp.float32) / half)
    angles = positions.astype(jnp.float32)[:, None] * freqs[None, :]
    cosine = jnp.cos(angles)[:, None, :]
    sine = jnp.sin(angles)[:, None, :]
    first = values[..., :half]
    second = values[..., half:]
    return jnp.concatenate([first * cosine - second * sine, first * sine + second * cosine], axis=-1)

def head_finish(values, gain, positions):
    normed = rms_scale(values, gain)
    return jnp.concatenate([normed[..., :NOPE], rotate(normed[..., NOPE:], positions)], axis=-1)

def reference(tokens, norm_gain, w_query_down, query_gain, w_query_up, w_latent_down, latent_gain, w_rotary_key, w_latent_up, query_head_gain, key_head_gain, w_pool_in, w_pool_mix, pool_scale, w_attn_out, w_pool_out, w_gate_attn, w_gate_pool):
    length = tokens.shape[0]
    bf = jnp.bfloat16
    positions = jnp.arange(length, dtype=jnp.int32)
    normed = rms_scale(tokens, norm_gain).astype(bf)
    query_latent = jnp.dot(normed, w_query_down, preferred_element_type=jnp.float32).astype(bf)
    query_normed = rms_scale(query_latent, query_gain).astype(bf)
    query_raw = jnp.dot(query_normed, w_query_up, preferred_element_type=jnp.float32).astype(bf)
    query_raw = query_raw.reshape(length, HEADS, NOPE + ROPE)
    query = (head_finish(query_raw, query_head_gain, positions) * (NOPE + ROPE) ** (-0.5)).astype(bf)
    latent = jnp.dot(normed, w_latent_down, preferred_element_type=jnp.float32).astype(bf)
    key_latent = rms_scale(latent, latent_gain).astype(bf)
    rotary_key = jnp.dot(normed, w_rotary_key, preferred_element_type=jnp.float32).astype(bf)
    keys_values = jnp.dot(key_latent, w_latent_up, preferred_element_type=jnp.float32).astype(bf)
    keys_values = keys_values.reshape(length, HEADS, NOPE + VALUE_DIM)
    key_raw = jnp.concatenate([keys_values[..., :NOPE], jnp.broadcast_to(rotary_key[:, None, :], (length, HEADS, ROPE))], axis=-1)
    key = head_finish(key_raw, key_head_gain, positions).astype(bf).astype(jnp.float32)
    values = keys_values[..., NOPE:].astype(jnp.float32)
    block = math.gcd(length, 256)
    query_blocks = query.reshape(length // block, block, HEADS, NOPE + ROPE)

    def attend(query_block):
        scores = jnp.einsum('qhd,khd->hqk', query_block.astype(jnp.float32), key)
        top = lax.optimization_barrier(jnp.max(scores, axis=-1, keepdims=True))
        expo = jnp.exp(scores - top)
        total = lax.optimization_barrier(jnp.sum(expo, axis=-1))
        rounded = lax.optimization_barrier(expo.astype(bf)).astype(jnp.float32)
        weighted = jnp.einsum('hqk,khv->qhv', rounded, values)
        return (weighted / jnp.transpose(total)[:, :, None]).astype(bf)
    attn_rows = lax.map(attend, query_blocks).reshape(length, HEADS * VALUE_DIM)
    pool_input = jnp.dot(normed, w_pool_in, preferred_element_type=jnp.float32).astype(bf)
    reach = 2 ** POOL_GROUPS // 2
    padded = jnp.pad(pool_input.astype(jnp.float32), ((reach, reach), (0, 0)))
    windows = jnp.power(2, jnp.arange(POOL_GROUPS, dtype=jnp.int32) + 1)
    channel_window = jnp.repeat(windows, POOL_GROUP)
    total = jnp.zeros((length, POOL_GROUPS * POOL_GROUP), jnp.float32)
    for shift in range(-reach, reach):
        inside = (shift >= -(channel_window // 2)) & (shift <= channel_window - channel_window // 2 - 1)
        total = total + jnp.where(inside[None, :], padded[reach + shift:reach + shift + length], 0.0)
    low = jnp.clip(positions[:, None] - channel_window[None, :] // 2, 0, length)
    high = jnp.clip(positions[:, None] + channel_window[None, :] - channel_window[None, :] // 2, 0, length)
    count = (high - low).astype(jnp.float32)
    pool_mixed = (total / count - pool_input.astype(jnp.float32)).astype(bf)
    pool_mixed = pool_mixed.reshape(length, POOL_GROUPS, POOL_GROUP)
    grouped = jnp.einsum('lgc,gcd->lgd', pool_mixed.astype(jnp.float32), w_pool_mix.astype(jnp.float32))
    pool_rows = (grouped.reshape(length, POOL_GROUPS * POOL_GROUP) * pool_scale).astype(bf)
    attn_branch = jnp.dot(attn_rows, w_attn_out, preferred_element_type=jnp.float32)
    pool_branch = jnp.dot(pool_rows, w_pool_out, preferred_element_type=jnp.float32)
    gate_attn = jax.nn.sigmoid(jnp.dot(normed, w_gate_attn, preferred_element_type=jnp.float32))
    gate_pool = jax.nn.sigmoid(jnp.dot(normed, w_gate_pool, preferred_element_type=jnp.float32))
    return (gate_attn * attn_branch + gate_pool * pool_branch).astype(bf)
```

```python
import functools
import math
import types

import jax
import numpy as np
import jax.numpy as jnp
from jax import lax
from jax.experimental import pallas as pl
from jax.experimental.pallas import tpu as pltpu
from jax.sharding import PartitionSpec as P

NOPE = 64
ROPE = 32
TURN = ROPE // 2
WIDTH = NOPE + ROPE
VALUE_DIM = 64
POOL_GROUPS = 4
POOL_GROUP = 256
LANES = 128
HALO = 16

eps = 1e-06
theta = 10000.0
f32 = jnp.float32
bf = jnp.bfloat16
MESH = pl.DeviceIdType.MESH
NT = (((1,), (1,)), ((), ()))


def flip(index, offset):
    bit = 1
    while bit <= offset:
        if offset & bit:
            index = index + bit - 2 * bit * ((index // bit) % 2)
        bit *= 2
    return index


def mm(a, b):
    return jnp.dot(a, b, preferred_element_type=f32)


def mm_nt(a, b):
    return lax.dot_general(a, b, NT, preferred_element_type=f32)


def phase(name):
    pass


def kernel(n, m, names, *refs):
    r = types.SimpleNamespace(**dict(zip(names, refs)))
    s = lax.axis_index("sp")
    t = lax.axis_index("tp")
    rows, cols = r.out.shape
    pairs = n // 2
    p = s // 2
    y = s % 2
    half = rows // 2
    across = flip(s, 1)
    twin = flip(t, 1)
    core = t % 2
    other = (s + n + 2 * y - 1) % n
    heads = r.queries.shape[0]
    rank = r.lat.shape[3]
    hc = cols // 2
    tiles = rows // LANES

    nearest = [
        sorted(range(pairs), key=lambda gap: (abs((q + gap) % pairs - q), gap)) for q in range(pairs)
    ]

    def gap_of(i):
        gap = jnp.int32(0)
        for q in range(pairs):
            if isinstance(i, int):
                mine_of = nearest[q][i]
            else:
                mine_of = jnp.int32(0)
                for k in range(1, pairs):
                    mine_of = mine_of + jnp.where(i == k, nearest[q][k], 0)
            gap = gap + jnp.where(p == q, mine_of, 0)
        return gap

    def same_parity(i):
        return ((p + i) % pairs) * 2 + y

    phase("barrier")
    barrier = pltpu.get_barrier_semaphore()
    peers = [(s, flip(t, off)) for off in range(1, m)]
    peers += [(same_parity(i), t) for i in range(1, pairs)]
    peers += [(across, t), (other, t)]
    for peer in peers:
        pl.semaphore_signal(barrier, inc=1, device_id=peer, device_id_type=MESH)

    def columns(block):
        return pl.ds(pl.multiple_of(block * cols, cols), cols)

    fetch = {}

    def take(name, src, dst, slot):
        copy = pltpu.make_async_copy(src, dst, r.local_sem.at[slot])
        copy.start()
        fetch.setdefault(name, []).append(copy)

    def have(*wanted):
        for name in wanted:
            for copy in fetch.pop(name, ()):
                copy.wait()

    take("tokens", r.h_tokens, r.tok.at[0], 0)
    mine = pl.ds(pl.multiple_of(t * cols, cols), cols)
    take("norm_gain", r.h_norm_gain, r.norm_gain, 1)
    take("w_latent_down", r.h_w_latent_down.at[mine, :], r.w_latent_down, 2)
    take("w_rotary", r.h_w_rotary.at[:, mine], r.w_rotary, 3)
    slot = 4
    for name in ("w_query_down", "w_gate_attn", "w_gate_pool", "w_pool_in"):
        for off in range(m):
            rows_of = pl.ds(pl.multiple_of(flip(t, off) * cols, cols), cols)
            place = pl.ds(off * cols, cols)
            source = getattr(r, "h_" + name).at[rows_of, :]
            take(name, source, getattr(r, name).at[place, :], slot)
        slot += 1
    for name in (
        "freqs",
        "w_query_up",
        "w_latent_up",
        "gain_q",
        "gain_k",
        "latent_gain",
        "query_gain",
        "w_pool_mix",
        "pool_scale",
    ):
        take("small", getattr(r, "h_" + name), getattr(r, name), slot)
    depth = r.wa.shape[2]
    for j in range(heads // 2):
        take("wa", r.h_attn_out.at[pl.ds(j * depth, depth), columns(t)], r.wa.at[j, 0], slot + 1)
    for o in range(m // 2):
        take("wp", r.h_pool_out.at[:, columns(flip(t, 2 * o))], r.wp.at[o, 0], slot + 2)

    def ready(off, start, size):
        base = flip(t, off) * cols + start
        raw = r.tok[off, :, start : start + size].astype(f32)
        gain = r.norm_gain[:, pl.ds(pl.multiple_of(base, hc), size)]
        spot = slice(off * cols + start, off * cols + start + size)
        r.scaled[:rows, spot] = (raw * gain).astype(bf)
        return jnp.sum(raw * raw, axis=-1, keepdims=True)

    def ready_edge(off):
        raw = r.edge[off].astype(f32)
        gain = r.norm_gain[:, columns(flip(t, off))]
        r.scaled[rows:, off * cols : (off + 1) * cols] = (raw * gain).astype(bf)
        return jnp.sum(raw * raw, axis=-1, keepdims=True)

    lane = lax.broadcasted_iota(jnp.int32, (1, LANES), 1)
    have("tokens", "norm_gain")
    squares = ready(0, 0, cols)
    have("w_latent_down", "w_rotary")
    part = mm(r.scaled[:rows, :cols], r.w_latent_down[...])
    side = mm_nt(r.scaled[:rows, :cols], r.w_rotary[...])
    side = jnp.concatenate([side, jnp.zeros((rows, LANES - ROPE), f32)], axis=1)
    side = jnp.where(lane == ROPE, squares, side)
    for e in range(2):
        r.sum_own[e, :, :rank] = part[e * half : (e + 1) * half]
        r.sum_own[e, :, rank:] = side[e * half : (e + 1) * half]
    pl.semaphore_wait(barrier, len(peers))

    def remote(src, dst, recv, peer):
        return pltpu.make_async_remote_copy(
            src_ref=src,
            dst_ref=dst,
            send_sem=r.sent,
            recv_sem=recv,
            device_id=peer,
            device_id_type=MESH,
        )

    def push(view, sem, off, least=1, most=m // 2):
        bit = most
        while bit >= least:
            if off == 0 or bit < (off & -off):
                slot = off ^ bit
                remote(view(off), view(slot), sem.at[slot - 1], (s, flip(t, bit))).start()
            bit //= 2

    def arrive(view, sem, off):
        remote(view(0), view(off), sem.at[off - 1], (s, t)).wait_recv()
        push(view, sem, off)

    def drain(view, sem):
        for slot in range(1, m):
            remote(view(0), view(slot), sem.at[slot - 1], (s, t)).wait_send()

    phase("push0")
    sum_copy = remote(r.sum_own.at[1 - core], r.sum_in, r.sum_sem, (s, twin))
    sum_copy.start()
    parts = 4
    width = cols // parts

    def tok_view(c):
        return lambda off: r.tok.at[off, :, pl.ds(c * width, width)]

    push(tok_view(0), r.tok_sem.at[0], 0, 2)
    downward = remote(
        r.tok.at[0, pl.ds(rows - HALO, HALO), :],
        r.edge.at[0, pl.ds(0, HALO), :],
        r.halo_sem.at[0],
        ((s + 1) % n, t),
    )
    upward = remote(
        r.tok.at[0, pl.ds(0, HALO), :],
        r.edge.at[0, pl.ds(HALO, HALO), :],
        r.halo_sem.at[1],
        ((s + n - 1) % n, t),
    )
    downward.start()
    upward.start()
    for c in range(parts):
        push(tok_view(c), r.tok_sem.at[c], 0, 1, 1)

    pair_copies = []
    for o in range(m // 2):
        pair_copies.append(
            remote(
                r.h_pool_out.at[:, columns(flip(twin, 2 * o))],
                r.wp.at[o, 1],
                r.wp_sem.at[o],
                (s, twin),
            )
        )
    for j in range(heads // 2):
        pair_copies.append(
            remote(
                r.h_attn_out.at[pl.ds(j * depth, depth), columns(twin)],
                r.wa.at[j, 1],
                r.wt_sem.at[j],
                (s, twin),
            )
        )
    for copy in pair_copies:
        copy.start()
    chunks = heads // 2
    share = chunks // 2

    def shared(half_of):
        return pl.ds(half_of * share, share)

    far_copies = []
    for off in range(2, m):
        for j in range(share):
            piece = y * share + j
            far_copies.append(
                remote(
                    r.h_attn_out.at[
                        pl.ds(pl.multiple_of(piece * depth, depth), depth), columns(flip(t, off))
                    ],
                    r.wa.at[piece, off],
                    r.wa_sem.at[off - 2, j],
                    (s, flip(t, off)),
                )
            )

    def over(off, j):
        piece = y * share + j
        return remote(
            r.wa.at[piece, off],
            r.wa.at[piece, off],
            r.wf_sem.at[off - 2, j],
            (across, t),
        )

    phase("own")

    def partial(off, w, start, size):
        spot = slice(off * cols + start, off * cols + start + size)
        return mm(r.scaled[:rows, spot], w[spot, :])

    def edge_view(off):
        return r.edge.at[off]

    wides = (
        ("w_query_down", r.acc_q, r.w_query_down),
        ("w_gate_attn", r.acc_ga, r.w_gate_attn),
        ("w_gate_pool", r.acc_gp, r.w_gate_pool),
        ("w_pool_in", r.acc_p, r.w_pool_in),
    )
    first = list(range(max(m // 2, 1)))
    later = list(range(max(m // 2, 1), m))
    for name, acc, w in wides[:1]:
        have(name)
        acc[...] = partial(0, w, 0, cols)

    phase("sum_pair")
    sum_copy.wait_recv()
    total = r.sum_own[core] + r.sum_in[...]
    side = jnp.concatenate([total[:, rank:], jnp.zeros((rank - half, LANES), f32)], axis=0).T
    row = lax.broadcasted_iota(jnp.int32, (TURN, rank), 0)
    levels = side[ROPE : ROPE + 1]
    coarse = levels.astype(bf).astype(f32)
    tail = jnp.where(row == 0, coarse, jnp.where(row == 1, levels - coarse, 0.0))
    r.sum_main[...] = total[:, :rank]
    r.sum_side[...] = side[: ROPE + 8]
    r.far_out[:half, :] = total[:, :rank].astype(bf)
    r.far_out[half : half + ROPE, :] = side[:ROPE].astype(bf)
    r.far_out[half + ROPE :, :] = tail.astype(bf)
    far_sums = []
    for off in range(2, m, 2):
        far_sums.append(
            remote(
                r.far_out,
                r.far_in.at[off // 2 - 1],
                r.fs_sem.at[off // 2 - 1],
                (s, flip(t, off)),
            )
        )
        far_sums[-1].start()
    for c in range(1, parts - 1):
        push(tok_view(c), r.tok_sem.at[c], 0, 2)

    phase("own2")
    for name, acc, w in wides[1:]:
        have(name)
        acc[...] = partial(0, w, 0, cols)
    phase("edge")
    downward.wait_recv()
    upward.wait_recv()
    push(edge_view, r.edge_sem, 0)
    push(tok_view(parts - 1), r.tok_sem.at[parts - 1], 0, 2)
    phase("own3")
    squares_edge = ready_edge(0)
    for off in first[1:]:
        for c in range(parts):
            arrive(tok_view(c), r.tok_sem.at[c], off)
        squares += ready(off, 0, cols)
        for name, acc, w in wides:
            acc[...] += partial(off, w, 0, cols)
    for off in first[1:]:
        arrive(edge_view, r.edge_sem, off)
        squares_edge += ready_edge(off)
    span = len(first) * cols
    r.acc_e[...] = mm(r.scaled[rows:, :span], r.w_pool_in[:span, :])

    phase("tables")
    have("small")
    freqs = jnp.concatenate([r.freqs[...]] * tiles, axis=1)
    along = lax.broadcasted_iota(jnp.int32, (ROPE, rows), 1)

    def table(k, carry):
        source = ((p + k // 2) % pairs) * 2 + (y + k) % 2
        angles = (source * rows + along[:TURN]).astype(f32) * freqs
        r.cosine[k] = jnp.cos(angles)
        r.sine[k] = jnp.sin(angles)
        return carry

    lax.fori_loop(0, n, table, 0)

    low = lane < NOPE
    spare = jnp.zeros((1, LANES - WIDTH), f32)
    turning = (lane >= NOPE) & (lane < WIDTH)

    def partner(values):
        swapped = jnp.where(
            lane < NOPE + TURN,
            pltpu.roll(values, LANES - TURN, 1),
            pltpu.roll(values, TURN, 1),
        )
        return jnp.where(turning, swapped, 0.0)

    gain_q = jnp.concatenate([r.gain_q[...], spare], axis=1)
    gain_q = gain_q * (WIDTH**-0.5 * math.log2(math.e))
    gain_q = jnp.broadcast_to(gain_q, (8, LANES))
    gain_p = partner(gain_q)
    side = jnp.zeros((LANES - WIDTH, rows), f32)
    cosine = jnp.concatenate([jnp.ones((NOPE, rows), f32), r.cosine[0], r.cosine[0], side], axis=0)
    sine = jnp.concatenate([jnp.zeros((NOPE, rows), f32), -r.sine[0], r.sine[0], side], axis=0)
    r.turn_q[0] = cosine.T * gain_q[:1]
    r.turn_q[1] = sine.T * gain_p[:1]
    gain_k = jnp.concatenate([r.gain_k[...], spare], axis=1)
    gain_k = jnp.broadcast_to(gain_k, (LANES, LANES)).T
    r.gain_rows[...] = jnp.concatenate([gain_k] * tiles, axis=1)

    for h in range(heads):
        up = r.w_query_up[:, h * WIDTH : (h + 1) * WIDTH].astype(f32)
        up = jnp.concatenate([up, jnp.zeros((up.shape[0], LANES - WIDTH), f32)], axis=1)
        r.up_q[:, h * LANES : (h + 1) * LANES] = up.astype(bf)
        r.up_q[:, (heads + h) * LANES : (heads + h + 1) * LANES] = partner(up).astype(bf)
    r.up_k[...] = r.w_latent_up[...].astype(f32).T.astype(bf)
    for e in range(2):
        for h in range(heads):
            r.keys[e, h, WIDTH:, :] = jnp.zeros((LANES - WIDTH, 2 * rows), bf)
            row = lax.broadcasted_iota(jnp.int32, (LANES - VALUE_DIM, 2 * rows), 0)
            r.values[e, h, VALUE_DIM:, :] = jnp.where(row == 0, 1.0, 0.0).astype(bf)
    r.attn_acc[...] = jnp.zeros_like(r.attn_acc)
    groups = r.w_pool_mix.shape[0]
    column = lax.broadcasted_iota(jnp.int32, (rows, rows + LANES), 1)
    before = (column >= rows) & (column < rows + HALO)
    column = jnp.where(before, column - rows - HALO, jnp.where(column < rows, column, column - HALO))
    apart = column - lax.broadcasted_iota(jnp.int32, (rows, rows + LANES), 0)
    place = s * rows + column
    exists = (place >= 0) & (place < rows * n)

    def reach_of(j):
        group = t * groups + j
        reach = jnp.int32(0)
        for i in range(POOL_GROUPS):
            reach = reach + jnp.where(group == i, 2**i, 0)
        return reach

    for j in range(groups):
        reach = reach_of(j)
        inside = exists & (apart >= -reach) & (apart <= reach - 1)
        r.band[j] = jnp.where(inside, 1.0, 0.0).astype(bf)
    pool = r.padded.shape[1]
    r.padded[pl.ds(rows + 2 * HALO, LANES - 2 * HALO), :] = jnp.zeros(
        (LANES - 2 * HALO, pool), bf
    )

    def rms(values, gain, width):
        mean = jnp.sum(values * values, axis=-1, keepdims=True) / width
        return values * lax.rsqrt(mean + eps) * gain

    phase("sum_far")
    main = r.sum_main[...]
    side = r.sum_side[:ROPE, :]
    levels = r.sum_side[ROPE : ROPE + 1, :]
    for i, copy in enumerate(far_sums):
        copy.wait_recv()
        main += r.far_in[i, :half, :].astype(f32)
        side += r.far_in[i, half : half + ROPE, :].astype(f32)
        tail = r.far_in[i, half + ROPE :, :].astype(f32)
        levels += tail[:1] + tail[1:2]
    level_row = lax.rsqrt(levels / (cols * m) + eps)
    level_column = jnp.broadcast_to(level_row, (LANES, rank)).T[:half, :1]
    latent = (main * level_column).astype(bf).astype(f32)
    r.lat[0, core, :half, :] = rms(latent, r.latent_gain[...], rank).astype(bf)
    r.lat[0, core, half:, :] = (side * level_row).astype(bf)

    near_copy = remote(
        r.lat.at[0, core], r.lat.at[1, core], r.main_sem.at[0], (across, t)
    )
    near_copy.start()
    for i in range(1, pairs):
        gap = (pairs - gap_of(i)) % pairs
        remote(
            r.lat.at[0, core],
            r.lat.at[2 * gap, core],
            r.main_sem.at[2 * gap - 1],
            (same_parity(pairs - gap), t),
        ).start()

    def main_wait(k):
        remote(
            r.lat.at[0, core], r.lat.at[k, core], r.main_sem.at[k - 1], (s, t)
        ).wait_recv()

    def to_across(k):
        return remote(
            r.lat.at[k, core], r.lat.at[k + 1, core], r.main_sem.at[k], (across, t)
        )

    def to_twin(k):
        return remote(
            r.lat.at[k, core], r.lat.at[k, core], r.pair_sem.at[k], (s, twin)
        )

    def twin_wait(k):
        remote(
            r.lat.at[k, core], r.lat.at[k, 1 - core], r.pair_sem.at[k], (s, twin)
        ).wait_recv()

    to_twin(0).start()

    def gather_tokens(h):
        total = 0.0
        for c in range(h * parts // 2, (h + 1) * parts // 2):
            for off in later:
                arrive(tok_view(c), r.tok_sem.at[c], off)
        if h == 1:
            for copy in far_copies:
                copy.start()
        for off in later:
            total += ready(off, h * hc, hc)
        return total

    def prepare(k, slot, e):
        latent = jnp.concatenate([r.lat[k, 0, :half, :], r.lat[k, 1, :half, :]], axis=0)

        def turns(part):
            got = r.lat[k, part, half:, :].astype(f32)
            return jnp.concatenate([got, jnp.zeros((ROPE, rows - rank), f32)], axis=1)

        whole = jnp.where(along < half, turns(0), pltpu.roll(turns(1), half, 1))
        x1 = whole[:TURN]
        x2 = whole[TURN:]
        shared_sum = jnp.sum(x1 * x1 + x2 * x2, axis=0, keepdims=True)
        x1 = x1 * r.gain_rows[NOPE : NOPE + TURN, :]
        x2 = x2 * r.gain_rows[NOPE + TURN : WIDTH, :]
        cosine = r.cosine[k]
        sine = r.sine[k]
        turn1 = x1 * cosine - x2 * sine
        turn2 = x1 * sine + x2 * cosine
        both = mm_nt(r.up_k[...], latent)
        spot = slice(e * rows, (e + 1) * rows)
        for h in range(heads):
            plain = both[h * LANES : h * LANES + NOPE].astype(bf).astype(f32)
            value = both[h * LANES + NOPE : (h + 1) * LANES].astype(bf)
            total = jnp.sum(plain * plain, axis=0, keepdims=True)
            level = lax.rsqrt((total + shared_sum) / WIDTH + eps)
            r.keys[slot, h, :NOPE, spot] = (plain * r.gain_rows[:NOPE, :] * level).astype(bf)
            r.keys[slot, h, NOPE : NOPE + TURN, spot] = (turn1 * level).astype(bf)
            r.keys[slot, h, NOPE + TURN : WIDTH, spot] = (turn2 * level).astype(bf)
            r.values[slot, h, :VALUE_DIM, spot] = value

    def attend(slot, h):
        scores = mm(r.queries[h], r.keys[slot, h])
        weighted = mm_nt(jnp.exp2(scores).astype(bf), r.values[slot, h])
        r.attn_acc[h] += weighted

    def forward(i):
        ahead = 2 * gap_of(i)
        main_wait(ahead)
        to_across(ahead).start()
        to_twin(ahead).start()

    def gather(i):
        now = 2 * gap_of(i)
        main_wait(now + 1)
        to_twin(now + 1).start()

    phase("later0")
    squares += gather_tokens(0)
    for name, acc, w in wides:
        total = acc[...]
        for off in later:
            total += partial(off, w, 0, hc)
        acc[...] = total

    phase("prep0")
    twin_wait(0)
    prepare(0, 0, 0)
    phase("wait_ahead")

    @pl.when(core == 1)
    def _():
        forward(1)

    phase("later1")
    for off in later:
        arrive(edge_view, r.edge_sem, off)
        squares_edge += ready_edge(off)
    r.acc_e[...] += mm(r.scaled[rows:, span:], r.w_pool_in[span:, :])
    squares += gather_tokens(1)
    scale = lax.rsqrt(squares / (cols * m) + eps)

    def finish(acc, w):
        total = acc[...]
        for off in later:
            total += partial(off, w, hc, hc)
        return total

    phase("pool_input")
    scale_edge = lax.rsqrt(squares_edge / (cols * m) + eps)
    r.padded[:rows, :] = (finish(r.acc_p, r.w_pool_in) * scale).astype(bf)
    r.padded[rows : rows + 2 * HALO, :] = (r.acc_e[...] * scale_edge).astype(bf)
    phase("pool")
    position = s * rows + lax.broadcasted_iota(jnp.int32, (rows, 1), 0)
    for j in range(groups):
        reach = reach_of(j)
        part = slice(j * POOL_GROUP, (j + 1) * POOL_GROUP)
        total = mm(r.band[j], r.padded[:, part])
        start = jnp.maximum(position - reach, 0)
        stop = jnp.minimum(position + reach, rows * n)
        count = (stop - start).astype(f32)
        own = r.padded[:rows, part].astype(f32)
        mixed = (total / count - own).astype(bf)
        r.prow[0, :, part] = (mm(mixed, r.w_pool_mix[j]) * r.pool_scale[:, part]).astype(bf)
    prow_copy = remote(r.prow.at[0], r.prow.at[1], r.pr_sem, (s, twin))
    prow_copy.start()
    phase("across0")
    gather(0)
    phase("ahead1")

    @pl.when(core == 0)
    def _():
        forward(1)

    phase("query")
    query_latent = (finish(r.acc_q, r.w_query_down) * scale).astype(bf).astype(f32)
    query_normed = rms(query_latent, r.query_gain[...], query_latent.shape[1]).astype(bf)
    query_raw = mm(query_normed, r.up_q[...])
    for h in range(heads):
        raw = query_raw[:, h * LANES : (h + 1) * LANES].astype(bf).astype(f32)
        swapped = query_raw[:, (heads + h) * LANES : (heads + h + 1) * LANES].astype(bf).astype(f32)
        mean = jnp.sum(raw * raw, axis=-1, keepdims=True) / WIDTH
        turned = raw * r.turn_q[0] + swapped * r.turn_q[1]
        r.queries[h] = (turned * lax.rsqrt(mean + eps)).astype(bf)

    phase("pool_out")
    prow_copy.wait_recv()
    have("wp")
    for o in range(m // 2):
        pair_copies[o].wait_recv()
    part_copies = []
    pool_rows = jnp.concatenate([r.prow[0], r.prow[1]], axis=1)
    for o in range(m // 2 - 1, -1, -1):
        weights = jnp.concatenate([r.wp[o, 0], r.wp[o, 1]], axis=0)
        branch = mm(pool_rows, weights)
        if o:
            r.psend[o - 1] = branch.astype(bf)
            copy = remote(
                r.psend.at[o - 1],
                r.precv.at[o - 1],
                r.pp_sem.at[o - 1],
                (s, flip(t, 2 * o)),
            )
            copy.start()
            part_copies.append(copy)
        else:
            r.acc_b[...] = branch

    phase("ahead2")
    if pairs > 2:
        forward(2)
    twin_wait(1)
    phase("pair0")
    prepare(1, 0, 1)
    for h in range(heads):
        attend(0, h)
    phase("across1")
    gather(1)
    phase("ahead3")
    if pairs > 3:
        forward(3)

    def relay():
        for off in range(2, m):
            for j in range(share):
                far_copies[(off - 2) * share + j].wait_recv()
                over(off, j).start()

    phase("steps")

    def step(i, carry):
        now = 2 * gap_of(i)

        @pl.when(i + 3 < pairs)
        def _():
            forward(i + 3)

        @pl.when(i == max(pairs - 4, 1))
        def _():
            relay()

        twin_wait(now)
        twin_wait(now + 1)
        prepare(now, i % 2, 0)
        prepare(now + 1, i % 2, 1)
        for h in range(chunks):
            attend(i % 2, h)
        gather(i + 1)
        for h in range(chunks, heads):
            attend(i % 2, h)
        return carry

    lax.fori_loop(1, pairs - 1, step, 0)

    phase("last_wait")
    i = pairs - 1
    now = 2 * gap_of(i)
    twin_wait(now)
    twin_wait(now + 1)
    phase("last_attend")
    prepare(now, i % 2, 0)
    prepare(now + 1, i % 2, 1)

    def rows_view(j):
        return lambda off: r.arows.at[j, off]

    for j in range(chunks):
        for h in (2 * j, 2 * j + 1):
            attend(i % 2, h)
        even = r.attn_acc[2 * j]
        odd = r.attn_acc[2 * j + 1]
        even = even / even[:, VALUE_DIM : VALUE_DIM + 1]
        odd = odd / odd[:, VALUE_DIM : VALUE_DIM + 1]
        r.arows[j, 0] = jnp.where(low, even, pltpu.roll(odd, VALUE_DIM, 1)).astype(bf)
        push(rows_view(j), r.ar_sem.at[j], 0)

    phase("gates")
    r.acc_ga[...] = lax.logistic(finish(r.acc_ga, r.w_gate_attn) * scale)
    r.acc_gp[...] = lax.logistic(finish(r.acc_gp, r.w_gate_pool) * scale)

    phase("pool_sum")
    branch = r.acc_b[...]
    for copy in part_copies:
        copy.wait_recv()
    for o in range(1, m // 2):
        branch += r.precv[o - 1].astype(f32)
    r.acc_gp[...] *= branch

    phase("w_wait")
    have("wa")
    for j in range(chunks):
        pair_copies[m // 2 + j].wait_recv()
    for off in range(2, m):
        for j in range(share):
            remote(
                r.wa.at[0, off],
                r.wa.at[(1 - y) * share + j, off],
                r.wf_sem.at[off - 2, j],
                (across, t),
            ).wait_recv()
    total = None
    for j in range(chunks):
        phase("rows%d" % j)
        for off in range(1, m):
            arrive(rows_view(j), r.ar_sem.at[j], off)
        phase("out%d" % j)
        left = jnp.concatenate([r.arows[j, off] for off in range(m)], axis=1)
        branch = mm(left, r.wa[j].reshape(m * depth, cols))
        total = branch if total is None else total + branch
    r.out[...] = (r.acc_ga[...] * total + r.acc_gp[...]).astype(bf)

    phase("drain")
    for c in range(parts):
        drain(tok_view(c), r.tok_sem.at[c])
    drain(edge_view, r.edge_sem)
    for j in range(chunks):
        drain(rows_view(j), r.ar_sem.at[j])
    for copy in pair_copies + far_copies + part_copies + far_sums + [sum_copy, prow_copy, downward, upward]:
        copy.wait_send()
    for off in range(2, m):
        for j in range(share):
            over(off, j).wait_send()
    for i in range(pairs):
        remote(r.lat.at[0, core], r.lat.at[0, core], r.main_sem.at[0], (s, t)).wait_send()
    for k in range(n):
        to_twin(k).wait_send()
        if k and k % 2 == 0:
            to_across(k).wait_send()
    phase(None)


def body(
    n,
    m,
    tokens,
    norm_gain,
    w_query_down,
    query_gain,
    w_query_up,
    w_latent_down,
    latent_gain,
    w_rotary_key,
    w_latent_up,
    query_head_gain,
    key_head_gain,
    w_pool_in,
    w_pool_mix,
    pool_scale,
    w_attn_out,
    w_pool_out,
    w_gate_attn,
    w_gate_pool,
):
    rows, cols = tokens.shape
    heads = w_query_up.shape[1] // WIDTH
    rank = w_latent_down.shape[1]
    qrank = w_query_down.shape[1]
    pool = w_pool_in.shape[1]
    groups = w_pool_mix.shape[0]
    chunks = heads // 2
    share = chunks // 2
    depth = w_attn_out.shape[0] // chunks
    freqs = np.repeat(theta ** (-np.arange(TURN) / TURN)[:, None], LANES, axis=1)
    dma = pltpu.SemaphoreType.DMA
    inputs = {
        "h_tokens": tokens,
        "h_norm_gain": norm_gain[None, :],
        "h_w_query_down": w_query_down,
        "h_query_gain": query_gain[None, :],
        "h_w_query_up": w_query_up,
        "h_w_latent_down": w_latent_down,
        "h_latent_gain": latent_gain[None, :],
        "h_w_rotary": w_rotary_key.T,
        "h_w_latent_up": w_latent_up,
        "h_gain_q": query_head_gain[None, :],
        "h_gain_k": key_head_gain[None, :],
        "h_w_pool_in": w_pool_in,
        "h_w_pool_mix": w_pool_mix,
        "h_pool_scale": pool_scale[None, :],
        "h_attn_out": w_attn_out,
        "h_pool_out": w_pool_out,
        "h_w_gate_attn": w_gate_attn,
        "h_w_gate_pool": w_gate_pool,
        "h_freqs": jnp.asarray(freqs, f32),
    }
    scratch = {}
    for name, value in inputs.items():
        if name not in ("h_tokens", "h_attn_out", "h_pool_out"):
            scratch[name[2:]] = pltpu.VMEM(value.shape, value.dtype)
    scratch["w_latent_down"] = pltpu.VMEM((cols, rank), bf)
    scratch["w_rotary"] = pltpu.VMEM((ROPE, cols), bf)
    scratch.update(
        tok=pltpu.VMEM((m, rows, cols), bf),
        scaled=pltpu.VMEM((rows + 2 * HALO, m * cols), bf),
        edge=pltpu.VMEM((m, 2 * HALO, cols), bf),
        acc_p=pltpu.VMEM((rows, pool), f32),
        acc_e=pltpu.VMEM((2 * HALO, pool), f32),
        wa=pltpu.VMEM((chunks, m, depth, cols), bf),
        wp=pltpu.VMEM((m // 2, 2, pool, cols), bf),
        acc_q=pltpu.VMEM((rows, qrank), f32),
        sum_own=pltpu.VMEM((2, rows // 2, rank + LANES), f32),
        sum_in=pltpu.VMEM((rows // 2, rank + LANES), f32),
        sum_main=pltpu.VMEM((rows // 2, rank), f32),
        sum_side=pltpu.VMEM((ROPE + 8, rank), f32),
        far_out=pltpu.VMEM((rows // 2 + ROPE + TURN, rank), bf),
        far_in=pltpu.VMEM((m // 2 - 1, rows // 2 + ROPE + TURN, rank), bf),
        acc_ga=pltpu.VMEM((rows, cols), f32),
        acc_gp=pltpu.VMEM((rows, cols), f32),
        acc_b=pltpu.VMEM((rows, cols), f32),
        cosine=pltpu.VMEM((n, TURN, rows), f32),
        sine=pltpu.VMEM((n, TURN, rows), f32),
        turn_q=pltpu.VMEM((2, rows, LANES), f32),
        gain_rows=pltpu.VMEM((LANES, rows), f32),
        up_q=pltpu.VMEM((qrank, 2 * heads * LANES), bf),
        up_k=pltpu.VMEM((heads * LANES, rank), bf),
        queries=pltpu.VMEM((heads, rows, LANES), bf),
        lat=pltpu.VMEM((n, 2, rows // 2 + ROPE, rank), bf),
        keys=pltpu.VMEM((2, heads, LANES, 2 * rows), bf),
        values=pltpu.VMEM((2, heads, LANES, 2 * rows), bf),
        attn_acc=pltpu.VMEM((heads, rows, LANES), f32),
        band=pltpu.VMEM((groups, rows, rows + LANES), bf),
        padded=pltpu.VMEM((rows + LANES, pool), bf),
        prow=pltpu.VMEM((2, rows, pool), bf),
        psend=pltpu.VMEM((m // 2 - 1, rows, cols), bf),
        precv=pltpu.VMEM((m // 2 - 1, rows, cols), bf),
        arows=pltpu.VMEM((chunks, m, rows, LANES), bf),
        local_sem=dma((11,)),
        sent=dma,
        tok_sem=dma((4, m - 1)),
        edge_sem=dma((m - 1,)),
        sum_sem=dma,
        fs_sem=dma((m // 2 - 1,)),
        wp_sem=dma((m // 2,)),
        wt_sem=dma((chunks,)),
        wa_sem=dma((m - 2, share)),
        wf_sem=dma((m - 2, share)),
        ar_sem=dma((chunks, m - 1)),
        pr_sem=dma,
        pp_sem=dma((m // 2 - 1,)),
        halo_sem=dma((2,)),
        main_sem=dma((n - 1,)),
        pair_sem=dma((n,)),
    )
    names = list(inputs) + ["out"] + list(scratch)
    return pl.pallas_call(
        functools.partial(kernel, n, m, names),
        out_shape=pltpu.VMEM((rows, cols), bf),
        in_specs=[pl.BlockSpec(memory_space=pl.ANY)] * len(inputs),
        out_specs=pl.BlockSpec(memory_space=pltpu.VMEM),
        scratch_shapes=list(scratch.values()),
        compiler_params=pltpu.CompilerParams(collective_id=0, has_side_effects=True),
    )(*inputs.values())


def solution(mesh):
    placed = (
        P("sp", "tp"),
        P(),
        P(),
        P(),
        P(None, "tp"),
        P(),
        P(),
        P(),
        P(None, "tp"),
        P(),
        P(),
        P(None, "tp"),
        P("tp", None, None),
        P("tp"),
        P("tp", None),
        P("tp", None),
        P(None, "tp"),
        P(None, "tp"),
    )
    held = functools.partial(body, mesh.shape["sp"], mesh.shape["tp"])
    return jax.shard_map(held, mesh=mesh, in_specs=placed, out_specs=P("sp", "tp"), check_vma=False)
```

```python
import functools
import math
import types

import jax
import numpy as np
import jax.numpy as jnp
from jax import lax
from jax.experimental import pallas as pl
from jax.experimental.pallas import tpu as pltpu
from jax.sharding import PartitionSpec as P

NOPE = 64
ROPE = 32
TURN = ROPE // 2
WIDTH = NOPE + ROPE
VALUE_DIM = 64
POOL_GROUPS = 4
POOL_GROUP = 256
LANES = 128
HALO = 8

eps = 1e-06
theta = 10000.0
f32 = jnp.float32
bf = jnp.bfloat16
MESH = pl.DeviceIdType.MESH
NT = (((1,), (1,)), ((), ()))


def flip(index, offset):
    bit = 1
    while bit <= offset:
        if offset & bit:
            index = index + bit - 2 * bit * ((index // bit) % 2)
        bit *= 2
    return index


def mm(a, b):
    return jnp.dot(a, b, preferred_element_type=f32)


def mm_nt(a, b):
    return lax.dot_general(a, b, NT, preferred_element_type=f32)


def phase(name):
    pass


def kernel(n, m, names, *refs):
    r = types.SimpleNamespace(**dict(zip(names, refs)))
    s = lax.axis_index("sp")
    t = lax.axis_index("tp")
    rows, cols = r.out.shape
    pairs = n // 2
    p = s // 2
    y = s % 2
    half = rows // 2
    across = flip(s, 1)
    twin = flip(t, 1)
    core = t % 2
    other = (s + n + 2 * y - 1) % n
    heads = r.queries.shape[0]
    rank = r.lat.shape[3]
    hc = cols // 2
    tiles = rows // LANES

    nearest = [
        sorted(range(pairs), key=lambda gap: (abs((q + gap) % pairs - q), gap)) for q in range(pairs)
    ]

    def gap_of(i):
        gap = jnp.int32(0)
        for q in range(pairs):
            if isinstance(i, int):
                mine_of = nearest[q][i]
            else:
                mine_of = jnp.int32(0)
                for k in range(1, pairs):
                    mine_of = mine_of + jnp.where(i == k, nearest[q][k], 0)
            gap = gap + jnp.where(p == q, mine_of, 0)
        return gap

    def same_parity(i):
        return ((p + i) % pairs) * 2 + y

    phase("barrier")
    barrier = pltpu.get_barrier_semaphore()
    peers = [(s, flip(t, off)) for off in range(1, m)]
    peers += [(same_parity(i), t) for i in range(1, pairs)]
    peers += [(across, t), (other, t)]
    for peer in peers:
        pl.semaphore_signal(barrier, inc=1, device_id=peer, device_id_type=MESH)

    def columns(block):
        return pl.ds(pl.multiple_of(block * cols, cols), cols)

    fetch = {}

    def take(name, src, dst, slot):
        copy = pltpu.make_async_copy(src, dst, r.local_sem.at[slot])
        copy.start()
        fetch.setdefault(name, []).append(copy)

    def have(*wanted):
        for name in wanted:
            for copy in fetch.pop(name, ()):
                copy.wait()

    take("tokens", r.h_tokens, r.tok.at[0], 0)
    mine = pl.ds(pl.multiple_of(t * cols, cols), cols)
    take("norm_gain", r.h_norm_gain, r.norm_gain, 1)
    take("w_latent_down", r.h_w_latent_down.at[mine, :], r.w_latent_down, 2)
    take("w_rotary", r.h_w_rotary.at[:, mine], r.w_rotary, 3)
    slot = 4
    for name in ("w_query_down", "w_gate_attn", "w_gate_pool", "w_pool_in"):
        for off in range(m):
            rows_of = pl.ds(pl.multiple_of(flip(t, off) * cols, cols), cols)
            place = pl.ds(off * cols, cols)
            source = getattr(r, "h_" + name).at[rows_of, :]
            take(name, source, getattr(r, name).at[place, :], slot)
        slot += 1
    for name in (
        "freqs",
        "w_query_up",
        "w_latent_up",
        "gain_q",
        "gain_k",
        "latent_gain",
        "query_gain",
        "w_pool_mix",
        "pool_scale",
    ):
        take("small", getattr(r, "h_" + name), getattr(r, name), slot)
    depth = r.wa.shape[2]
    for j in range(heads // 2):
        take("wa", r.h_attn_out.at[pl.ds(j * depth, depth), columns(t)], r.wa.at[j, 0], slot + 1)
    for o in range(m // 2):
        take("wp", r.h_pool_out.at[:, columns(flip(t, 2 * o))], r.wp.at[o, 0], slot + 2)

    def ready(off, start, size):
        base = flip(t, off) * cols + start
        raw = r.tok[off, :, start : start + size].astype(f32)
        gain = r.norm_gain[:, pl.ds(pl.multiple_of(base, hc), size)]
        spot = slice(off * cols + start, off * cols + start + size)
        r.scaled[:rows, spot] = (raw * gain).astype(bf)
        return jnp.sum(raw * raw, axis=-1, keepdims=True)

    def ready_edge(off):
        raw = r.edge[off].astype(f32)
        gain = r.norm_gain[:, columns(flip(t, off))]
        r.scaled[rows:, off * cols : (off + 1) * cols] = (raw * gain).astype(bf)
        return jnp.sum(raw * raw, axis=-1, keepdims=True)

    lane = lax.broadcasted_iota(jnp.int32, (1, LANES), 1)
    have("tokens", "norm_gain")
    squares = ready(0, 0, cols)
    have("w_latent_down", "w_rotary")
    part = mm(r.scaled[:rows, :cols], r.w_latent_down[...])
    side = mm_nt(r.scaled[:rows, :cols], r.w_rotary[...])
    side = jnp.concatenate([side, jnp.zeros((rows, LANES - ROPE), f32)], axis=1)
    side = jnp.where(lane == ROPE, squares, side)
    for e in range(2):
        r.sum_own[e, :, :rank] = part[e * half : (e + 1) * half]
        r.sum_own[e, :, rank:] = side[e * half : (e + 1) * half]
    pl.semaphore_wait(barrier, len(peers))

    def remote(src, dst, recv, peer):
        return pltpu.make_async_remote_copy(
            src_ref=src,
            dst_ref=dst,
            send_sem=r.sent,
            recv_sem=recv,
            device_id=peer,
            device_id_type=MESH,
        )

    def push(view, sem, off, least=1, most=m // 2):
        bit = most
        while bit >= least:
            if off == 0 or bit < (off & -off):
                slot = off ^ bit
                remote(view(off), view(slot), sem.at[slot - 1], (s, flip(t, bit))).start()
            bit //= 2

    def arrive(view, sem, off):
        remote(view(0), view(off), sem.at[off - 1], (s, t)).wait_recv()
        push(view, sem, off)

    def drain(view, sem):
        for slot in range(1, m):
            remote(view(0), view(slot), sem.at[slot - 1], (s, t)).wait_send()

    phase("push0")
    sum_copy = remote(r.sum_own.at[1 - core], r.sum_in, r.sum_sem, (s, twin))
    sum_copy.start()
    parts = 4
    width = cols // parts

    def tok_view(c):
        return lambda off: r.tok.at[off, :, pl.ds(c * width, width)]

    push(tok_view(0), r.tok_sem.at[0], 0, 2)
    downward = remote(
        r.tok.at[0, pl.ds(rows - HALO, HALO), :],
        r.edge.at[0, pl.ds(0, HALO), :],
        r.halo_sem.at[0],
        ((s + 1) % n, t),
    )
    upward = remote(
        r.tok.at[0, pl.ds(0, HALO), :],
        r.edge.at[0, pl.ds(HALO, HALO), :],
        r.halo_sem.at[1],
        ((s + n - 1) % n, t),
    )
    downward.start()
    upward.start()
    for c in range(parts):
        push(tok_view(c), r.tok_sem.at[c], 0, 1, 1)

    pair_copies = []
    for o in range(m // 2):
        pair_copies.append(
            remote(
                r.h_pool_out.at[:, columns(flip(twin, 2 * o))],
                r.wp.at[o, 1],
                r.wp_sem.at[o],
                (s, twin),
            )
        )
    for j in range(heads // 2):
        pair_copies.append(
            remote(
                r.h_attn_out.at[pl.ds(j * depth, depth), columns(twin)],
                r.wa.at[j, 1],
                r.wt_sem.at[j],
                (s, twin),
            )
        )
    for copy in pair_copies:
        copy.start()
    chunks = heads // 2
    share = chunks // 2

    def shared(half_of):
        return pl.ds(half_of * share, share)

    beside = flip(s, 2)
    level = p % 2
    slab = depth // 2

    def slab_rows(start, which):
        return pl.ds(pl.multiple_of(start + which * slab, slab), slab)

    far_copies = []
    for off in range(2, m):
        for j in range(share):
            piece = y * share + j
            far_copies.append(
                remote(
                    r.h_attn_out.at[slab_rows(piece * depth, level), columns(flip(t, off))],
                    r.wa.at[piece, off, slab_rows(0, level)],
                    r.wa_sem.at[off - 2, j],
                    (s, flip(t, off)),
                )
            )

    def along_line(off, j):
        part = r.wa.at[y * share + j, off, slab_rows(0, level)]
        return remote(part, part, r.wz_sem.at[off - 2, j], (beside, t))

    def over(off, j):
        piece = r.wa.at[y * share + j, off]
        return remote(piece, piece, r.wf_sem.at[off - 2, j], (across, t))

    phase("own")

    def partial(off, w, start, size):
        spot = slice(off * cols + start, off * cols + start + size)
        return mm(r.scaled[:rows, spot], w[spot, :])

    def edge_view(off):
        return r.edge.at[off]

    wides = (
        ("w_query_down", r.acc_q, r.w_query_down),
        ("w_gate_attn", r.acc_ga, r.w_gate_attn),
        ("w_gate_pool", r.acc_gp, r.w_gate_pool),
        ("w_pool_in", r.acc_p, r.w_pool_in),
    )
    first = list(range(max(m // 2, 1)))
    later = list(range(max(m // 2, 1), m))
    for name, acc, w in wides[:1]:
        have(name)
        acc[...] = partial(0, w, 0, cols)

    phase("sum_pair")
    sum_copy.wait_recv()
    total = r.sum_own[core] + r.sum_in[...]
    side = jnp.concatenate([total[:, rank:], jnp.zeros((rank - half, LANES), f32)], axis=0).T
    row = lax.broadcasted_iota(jnp.int32, (TURN, rank), 0)
    levels = side[ROPE : ROPE + 1]
    coarse = levels.astype(bf).astype(f32)
    tail = jnp.where(row == 0, coarse, jnp.where(row == 1, levels - coarse, 0.0))
    r.sum_main[...] = total[:, :rank]
    r.sum_side[...] = side[: ROPE + 8]
    r.far_out[:half, :] = total[:, :rank].astype(bf)
    r.far_out[half : half + ROPE, :] = side[:ROPE].astype(bf)
    r.far_out[half + ROPE :, :] = tail.astype(bf)
    far_sums = []
    for off in range(2, m, 2):
        far_sums.append(
            remote(
                r.far_out,
                r.far_in.at[off // 2 - 1],
                r.fs_sem.at[off // 2 - 1],
                (s, flip(t, off)),
            )
        )
        far_sums[-1].start()
    for c in range(1, parts - 1):
        push(tok_view(c), r.tok_sem.at[c], 0, 2)

    phase("own2")
    for name, acc, w in wides[1:]:
        have(name)
        acc[...] = partial(0, w, 0, cols)
    phase("edge")
    downward.wait_recv()
    upward.wait_recv()
    push(edge_view, r.edge_sem, 0)
    push(tok_view(parts - 1), r.tok_sem.at[parts - 1], 0, 2)
    phase("own3")
    squares_edge = ready_edge(0)
    for off in first[1:]:
        for c in range(parts):
            arrive(tok_view(c), r.tok_sem.at[c], off)
        squares += ready(off, 0, cols)
        for name, acc, w in wides:
            acc[...] += partial(off, w, 0, cols)
    for off in first[1:]:
        arrive(edge_view, r.edge_sem, off)
        squares_edge += ready_edge(off)
    span = len(first) * cols
    r.acc_e[...] = mm(r.scaled[rows:, :span], r.w_pool_in[:span, :])

    have("small")

    def rms(values, gain, width):
        mean = jnp.sum(values * values, axis=-1, keepdims=True) / width
        return values * lax.rsqrt(mean + eps) * gain

    phase("sum_far")
    main = r.sum_main[...]
    side = r.sum_side[:ROPE, :]
    levels = r.sum_side[ROPE : ROPE + 1, :]
    for i, copy in enumerate(far_sums):
        copy.wait_recv()
        main += r.far_in[i, :half, :].astype(f32)
        side += r.far_in[i, half : half + ROPE, :].astype(f32)
        tail = r.far_in[i, half + ROPE :, :].astype(f32)
        levels += tail[:1] + tail[1:2]
    level_row = lax.rsqrt(levels / (cols * m) + eps)
    level_column = jnp.broadcast_to(level_row, (LANES, rank)).T[:half, :1]
    latent = (main * level_column).astype(bf).astype(f32)
    r.lat[0, core, :half, :] = rms(latent, r.latent_gain[...], rank).astype(bf)
    r.lat[0, core, half:, :] = (side * level_row).astype(bf)

    near_copy = remote(
        r.lat.at[0, core], r.lat.at[1, core], r.main_sem.at[0], (across, t)
    )
    near_copy.start()

    def send(i):
        gap = (pairs - gap_of(i)) % pairs
        remote(
            r.lat.at[0, core],
            r.lat.at[2 * gap, core],
            r.main_sem.at[2 * gap - 1],
            (same_parity(pairs - gap), t),
        ).start()

    inner = (p > 0) & (p < pairs - 1)
    outer = jnp.logical_not(inner)
    head = p == 0
    tail_end = p == pairs - 1

    def only(condition, act, i):
        if i < pairs:

            @pl.when(condition)
            def _():
                act(i)

    send(1)
    only(inner, send, 2)

    def main_wait(k):
        remote(
            r.lat.at[0, core], r.lat.at[k, core], r.main_sem.at[k - 1], (s, t)
        ).wait_recv()

    def to_across(k):
        return remote(
            r.lat.at[k, core], r.lat.at[k + 1, core], r.main_sem.at[k], (across, t)
        )

    def to_twin(k):
        return remote(
            r.lat.at[k, core], r.lat.at[k, core], r.pair_sem.at[k], (s, twin)
        )

    def twin_wait(k):
        remote(
            r.lat.at[k, core], r.lat.at[k, 1 - core], r.pair_sem.at[k], (s, twin)
        ).wait_recv()

    to_twin(0).start()

    phase("tables")
    freqs = jnp.concatenate([r.freqs[...]] * tiles, axis=1)
    along = lax.broadcasted_iota(jnp.int32, (ROPE, rows), 1)

    def table(k, carry):
        source = ((p + k // 2) % pairs) * 2 + (y + k) % 2
        angles = (source * rows + along[:TURN]).astype(f32) * freqs
        r.cosine[k] = jnp.cos(angles)
        r.sine[k] = jnp.sin(angles)
        return carry

    lax.fori_loop(0, n, table, 0)

    low = lane < NOPE
    spare = jnp.zeros((1, LANES - WIDTH), f32)
    turning = (lane >= NOPE) & (lane < WIDTH)

    def partner(values):
        swapped = jnp.where(
            lane < NOPE + TURN,
            pltpu.roll(values, LANES - TURN, 1),
            pltpu.roll(values, TURN, 1),
        )
        return jnp.where(turning, swapped, 0.0)

    gain_q = jnp.concatenate([r.gain_q[...], spare], axis=1)
    gain_q = gain_q * (WIDTH**-0.5 * math.log2(math.e))
    gain_q = jnp.broadcast_to(gain_q, (8, LANES))
    gain_p = partner(gain_q)
    side = jnp.zeros((LANES - WIDTH, rows), f32)
    cosine = jnp.concatenate([jnp.ones((NOPE, rows), f32), r.cosine[0], r.cosine[0], side], axis=0)
    sine = jnp.concatenate([jnp.zeros((NOPE, rows), f32), -r.sine[0], r.sine[0], side], axis=0)
    r.turn_q[0] = cosine.T * gain_q[:1]
    r.turn_q[1] = sine.T * gain_p[:1]
    gain_k = jnp.concatenate([r.gain_k[...], spare], axis=1)
    gain_k = jnp.broadcast_to(gain_k, (LANES, LANES)).T
    r.gain_rows[...] = jnp.concatenate([gain_k] * tiles, axis=1)

    for h in range(heads):
        up = r.w_query_up[:, h * WIDTH : (h + 1) * WIDTH].astype(f32)
        up = jnp.concatenate([up, jnp.zeros((up.shape[0], LANES - WIDTH), f32)], axis=1)
        r.up_q[:, h * LANES : (h + 1) * LANES] = up.astype(bf)
        r.up_q[:, (heads + h) * LANES : (heads + h + 1) * LANES] = partner(up).astype(bf)
    r.up_k[...] = r.w_latent_up[...].astype(f32).T.astype(bf)
    for e in range(2):
        for h in range(heads):
            r.keys[e, h, WIDTH:, :] = jnp.zeros((LANES - WIDTH, 2 * rows), bf)
            row = lax.broadcasted_iota(jnp.int32, (LANES - VALUE_DIM, 2 * rows), 0)
            r.values[e, h, VALUE_DIM:, :] = jnp.where(row == 0, 1.0, 0.0).astype(bf)
    r.attn_acc[...] = jnp.zeros_like(r.attn_acc)
    groups = r.w_pool_mix.shape[0]
    column = lax.broadcasted_iota(jnp.int32, (rows, rows + LANES), 1)
    before = (column >= rows) & (column < rows + HALO)
    column = jnp.where(before, column - rows - HALO, jnp.where(column < rows, column, column - HALO))
    apart = column - lax.broadcasted_iota(jnp.int32, (rows, rows + LANES), 0)
    place = s * rows + column
    exists = (place >= 0) & (place < rows * n)

    def reach_of(j):
        group = t * groups + j
        reach = jnp.int32(0)
        for i in range(POOL_GROUPS):
            reach = reach + jnp.where(group == i, 2**i, 0)
        return reach

    for j in range(groups):
        reach = reach_of(j)
        inside = exists & (apart >= -reach) & (apart <= reach - 1)
        r.band[j] = jnp.where(inside, 1.0, 0.0).astype(bf)
    pool = r.padded.shape[1]
    r.padded[pl.ds(rows + 2 * HALO, LANES - 2 * HALO), :] = jnp.zeros(
        (LANES - 2 * HALO, pool), bf
    )

    def gather_tokens(h):
        total = 0.0
        for c in range(h * parts // 2, (h + 1) * parts // 2):
            for off in later:
                arrive(tok_view(c), r.tok_sem.at[c], off)
            if c == 0:
                only(head, send, 2)
                only(jnp.logical_not(head), send, 3)
            if c == parts // 2:
                only(head, send, 3)
                only(tail_end, send, 2)
                for i in range(4, pairs):
                    send(i)
                for copy in far_copies:
                    copy.start()
                only(inner, forward, 2)
        for off in later:
            total += ready(off, h * hc, hc)
        return total

    def prepare(k, slot, e):
        latent = jnp.concatenate([r.lat[k, 0, :half, :], r.lat[k, 1, :half, :]], axis=0)

        def turns(part):
            got = r.lat[k, part, half:, :].astype(f32)
            return jnp.concatenate([got, jnp.zeros((ROPE, rows - rank), f32)], axis=1)

        whole = jnp.where(along < half, turns(0), pltpu.roll(turns(1), half, 1))
        x1 = whole[:TURN]
        x2 = whole[TURN:]
        shared_sum = jnp.sum(x1 * x1 + x2 * x2, axis=0, keepdims=True)
        x1 = x1 * r.gain_rows[NOPE : NOPE + TURN, :]
        x2 = x2 * r.gain_rows[NOPE + TURN : WIDTH, :]
        cosine = r.cosine[k]
        sine = r.sine[k]
        turn1 = x1 * cosine - x2 * sine
        turn2 = x1 * sine + x2 * cosine
        both = mm_nt(r.up_k[...], latent)
        spot = slice(e * rows, (e + 1) * rows)
        for h in range(heads):
            plain = both[h * LANES : h * LANES + NOPE].astype(bf).astype(f32)
            value = both[h * LANES + NOPE : (h + 1) * LANES].astype(bf)
            total = jnp.sum(plain * plain, axis=0, keepdims=True)
            level = lax.rsqrt((total + shared_sum) / WIDTH + eps)
            r.keys[slot, h, :NOPE, spot] = (plain * r.gain_rows[:NOPE, :] * level).astype(bf)
            r.keys[slot, h, NOPE : NOPE + TURN, spot] = (turn1 * level).astype(bf)
            r.keys[slot, h, NOPE + TURN : WIDTH, spot] = (turn2 * level).astype(bf)
            r.values[slot, h, :VALUE_DIM, spot] = value

    def attend(slot, h):
        scores = mm(r.queries[h], r.keys[slot, h])
        weighted = mm_nt(jnp.exp2(scores).astype(bf), r.values[slot, h])
        r.attn_acc[h] += weighted

    def forward(i):
        ahead = 2 * gap_of(i)
        main_wait(ahead)
        to_across(ahead).start()
        to_twin(ahead).start()

    def gather(i):
        now = 2 * gap_of(i)
        main_wait(now + 1)
        to_twin(now + 1).start()

    phase("later0")
    squares += gather_tokens(0)
    for name, acc, w in wides:
        total = acc[...]
        for off in later:
            total += partial(off, w, 0, hc)
        acc[...] = total

    phase("prep0")
    twin_wait(0)
    prepare(0, 0, 0)
    phase("across0")
    gather(0)
    phase("ahead1")
    forward(1)
    phase("later1")
    for off in later:
        arrive(edge_view, r.edge_sem, off)
        squares_edge += ready_edge(off)
    r.acc_e[...] += mm(r.scaled[rows:, span:], r.w_pool_in[span:, :])
    squares += gather_tokens(1)
    scale = lax.rsqrt(squares / (cols * m) + eps)

    def finish(acc, w):
        total = acc[...]
        for off in later:
            total += partial(off, w, hc, hc)
        return total

    phase("pool_input")
    scale_edge = lax.rsqrt(squares_edge / (cols * m) + eps)
    r.padded[:rows, :] = (finish(r.acc_p, r.w_pool_in) * scale).astype(bf)
    r.padded[rows : rows + 2 * HALO, :] = (r.acc_e[...] * scale_edge).astype(bf)
    phase("pool")
    position = s * rows + lax.broadcasted_iota(jnp.int32, (rows, 1), 0)
    for j in range(groups):
        reach = reach_of(j)
        part = slice(j * POOL_GROUP, (j + 1) * POOL_GROUP)
        total = mm(r.band[j], r.padded[:, part])
        start = jnp.maximum(position - reach, 0)
        stop = jnp.minimum(position + reach, rows * n)
        count = (stop - start).astype(f32)
        own = r.padded[:rows, part].astype(f32)
        mixed = (total / count - own).astype(bf)
        r.prow[0, :, part] = (mm(mixed, r.w_pool_mix[j]) * r.pool_scale[:, part]).astype(bf)
    prow_copy = remote(r.prow.at[0], r.prow.at[1], r.pr_sem, (s, twin))
    prow_copy.start()
    phase("query")
    query_latent = (finish(r.acc_q, r.w_query_down) * scale).astype(bf).astype(f32)
    query_normed = rms(query_latent, r.query_gain[...], query_latent.shape[1]).astype(bf)
    query_raw = mm(query_normed, r.up_q[...])
    for h in range(heads):
        raw = query_raw[:, h * LANES : (h + 1) * LANES].astype(bf).astype(f32)
        swapped = query_raw[:, (heads + h) * LANES : (heads + h + 1) * LANES].astype(bf).astype(f32)
        mean = jnp.sum(raw * raw, axis=-1, keepdims=True) / WIDTH
        turned = raw * r.turn_q[0] + swapped * r.turn_q[1]
        r.queries[h] = (turned * lax.rsqrt(mean + eps)).astype(bf)

    phase("ahead2")
    only(outer, forward, 2)
    only(jnp.logical_not(tail_end), forward, 3)
    def relay_line():
        for off in range(2, m):
            for j in range(share):
                far_copies[(off - 2) * share + j].wait_recv()
                along_line(off, j).start()

    phase("across1")
    gather(1)
    phase("pool_out")
    prow_copy.wait_recv()
    have("wp")
    for o in range(m // 2):
        pair_copies[o].wait_recv()
    part_copies = []
    pool_rows = jnp.concatenate([r.prow[0], r.prow[1]], axis=1)
    for o in range(m // 2 - 1, -1, -1):
        weights = jnp.concatenate([r.wp[o, 0], r.wp[o, 1]], axis=0)
        branch = mm(pool_rows, weights)
        if o:
            r.psend[o - 1] = branch.astype(bf)
            copy = remote(
                r.psend.at[o - 1],
                r.precv.at[o - 1],
                r.pp_sem.at[o - 1],
                (s, flip(t, 2 * o)),
            )
            copy.start()
            part_copies.append(copy)
        else:
            r.acc_b[...] = branch

    phase("relay_line")
    relay_line()
    phase("pair0")
    twin_wait(1)
    prepare(1, 0, 1)
    for h in range(heads):
        attend(0, h)
    phase("ahead3")
    only(tail_end, forward, 3)
    def relay():
        for off in range(2, m):
            for j in range(share):
                remote(
                    r.wa.at[y * share + j, off, slab_rows(0, level)],
                    r.wa.at[y * share + j, off, slab_rows(0, 1 - level)],
                    r.wz_sem.at[off - 2, j],
                    (beside, t),
                ).wait_recv()
                over(off, j).start()

    phase("steps")

    def step(i, carry):
        now = 2 * gap_of(i)

        @pl.when(i + 3 < pairs)
        def _():
            forward(i + 3)

        twin_wait(now)
        twin_wait(now + 1)
        prepare(now, i % 2, 0)
        prepare(now + 1, i % 2, 1)
        for h in range(chunks):
            attend(i % 2, h)
        gather(i + 1)

        @pl.when(i == pairs - 2)
        def _():
            relay()

        for h in range(chunks, heads):
            attend(i % 2, h)
        return carry

    lax.fori_loop(1, pairs - 1, step, 0)

    phase("last_wait")
    i = pairs - 1
    now = 2 * gap_of(i)
    twin_wait(now)
    twin_wait(now + 1)
    phase("last_attend")
    prepare(now, i % 2, 0)
    prepare(now + 1, i % 2, 1)

    def rows_view(j):
        return lambda off: r.arows.at[j, off]

    order = [y * share + j for j in range(share)] + [(1 - y) * share + j for j in range(share)]
    for j, chunk in enumerate(order):
        for h in (2 * chunk, 2 * chunk + 1):
            attend(i % 2, h)
        even = r.attn_acc[2 * chunk]
        odd = r.attn_acc[2 * chunk + 1]
        even = even / even[:, VALUE_DIM : VALUE_DIM + 1]
        odd = odd / odd[:, VALUE_DIM : VALUE_DIM + 1]
        r.arows[j, 0] = jnp.where(low, even, pltpu.roll(odd, VALUE_DIM, 1)).astype(bf)
        push(rows_view(j), r.ar_sem.at[j], 0)

    phase("gates")
    r.acc_ga[...] = lax.logistic(finish(r.acc_ga, r.w_gate_attn) * scale)
    r.acc_gp[...] = lax.logistic(finish(r.acc_gp, r.w_gate_pool) * scale)

    phase("pool_sum")
    branch = r.acc_b[...]
    for copy in part_copies:
        copy.wait_recv()
    for o in range(1, m // 2):
        branch += r.precv[o - 1].astype(f32)
    r.acc_gp[...] *= branch

    phase("w_wait")
    have("wa")
    for j in range(chunks):
        pair_copies[m // 2 + j].wait_recv()
    total = None
    for j in range(chunks):
        phase("rows%d" % j)
        for off in range(1, m - 1):
            arrive(rows_view(j), r.ar_sem.at[j], off)
        if j == share:
            for off in range(2, m):
                for k in range(share):
                    remote(
                        r.wa.at[0, off],
                        r.wa.at[(1 - y) * share + k, off],
                        r.wf_sem.at[off - 2, k],
                        (across, t),
                    ).wait_recv()
        left = jnp.concatenate([r.arows[j, off] for off in range(m - 1)], axis=1)
        branch = mm(left, r.wa[order[j], : m - 1].reshape((m - 1) * depth, cols))
        total = branch if total is None else total + branch
        arrive(rows_view(j), r.ar_sem.at[j], m - 1)
        phase("out%d" % j)
        total += mm(r.arows[j, m - 1], r.wa[order[j], m - 1])
    r.out[...] = (r.acc_ga[...] * total + r.acc_gp[...]).astype(bf)

    phase("drain")
    for c in range(parts):
        drain(tok_view(c), r.tok_sem.at[c])
    drain(edge_view, r.edge_sem)
    for j in range(chunks):
        drain(rows_view(j), r.ar_sem.at[j])
    for copy in pair_copies + far_copies + part_copies + far_sums + [sum_copy, prow_copy, downward, upward]:
        copy.wait_send()
    for off in range(2, m):
        for j in range(share):
            over(off, j).wait_send()
            along_line(off, j).wait_send()
    for i in range(pairs):
        remote(r.lat.at[0, core], r.lat.at[0, core], r.main_sem.at[0], (s, t)).wait_send()
    for k in range(n):
        to_twin(k).wait_send()
        if k and k % 2 == 0:
            to_across(k).wait_send()
    phase(None)


def body(
    n,
    m,
    tokens,
    norm_gain,
    w_query_down,
    query_gain,
    w_query_up,
    w_latent_down,
    latent_gain,
    w_rotary_key,
    w_latent_up,
    query_head_gain,
    key_head_gain,
    w_pool_in,
    w_pool_mix,
    pool_scale,
    w_attn_out,
    w_pool_out,
    w_gate_attn,
    w_gate_pool,
):
    rows, cols = tokens.shape
    heads = w_query_up.shape[1] // WIDTH
    rank = w_latent_down.shape[1]
    qrank = w_query_down.shape[1]
    pool = w_pool_in.shape[1]
    groups = w_pool_mix.shape[0]
    chunks = heads // 2
    share = chunks // 2
    depth = w_attn_out.shape[0] // chunks
    freqs = np.repeat(theta ** (-np.arange(TURN) / TURN)[:, None], LANES, axis=1)
    dma = pltpu.SemaphoreType.DMA
    inputs = {
        "h_tokens": tokens,
        "h_norm_gain": norm_gain[None, :],
        "h_w_query_down": w_query_down,
        "h_query_gain": query_gain[None, :],
        "h_w_query_up": w_query_up,
        "h_w_latent_down": w_latent_down,
        "h_latent_gain": latent_gain[None, :],
        "h_w_rotary": w_rotary_key.T,
        "h_w_latent_up": w_latent_up,
        "h_gain_q": query_head_gain[None, :],
        "h_gain_k": key_head_gain[None, :],
        "h_w_pool_in": w_pool_in,
        "h_w_pool_mix": w_pool_mix,
        "h_pool_scale": pool_scale[None, :],
        "h_attn_out": w_attn_out,
        "h_pool_out": w_pool_out,
        "h_w_gate_attn": w_gate_attn,
        "h_w_gate_pool": w_gate_pool,
        "h_freqs": jnp.asarray(freqs, f32),
    }
    scratch = {}
    for name, value in inputs.items():
        if name not in ("h_tokens", "h_attn_out", "h_pool_out"):
            scratch[name[2:]] = pltpu.VMEM(value.shape, value.dtype)
    scratch["w_latent_down"] = pltpu.VMEM((cols, rank), bf)
    scratch["w_rotary"] = pltpu.VMEM((ROPE, cols), bf)
    scratch.update(
        tok=pltpu.VMEM((m, rows, cols), bf),
        scaled=pltpu.VMEM((rows + 2 * HALO, m * cols), bf),
        edge=pltpu.VMEM((m, 2 * HALO, cols), bf),
        acc_p=pltpu.VMEM((rows, pool), f32),
        acc_e=pltpu.VMEM((2 * HALO, pool), f32),
        wa=pltpu.VMEM((chunks, m, depth, cols), bf),
        wp=pltpu.VMEM((m // 2, 2, pool, cols), bf),
        acc_q=pltpu.VMEM((rows, qrank), f32),
        sum_own=pltpu.VMEM((2, rows // 2, rank + LANES), f32),
        sum_in=pltpu.VMEM((rows // 2, rank + LANES), f32),
        sum_main=pltpu.VMEM((rows // 2, rank), f32),
        sum_side=pltpu.VMEM((ROPE + 8, rank), f32),
        far_out=pltpu.VMEM((rows // 2 + ROPE + TURN, rank), bf),
        far_in=pltpu.VMEM((m // 2 - 1, rows // 2 + ROPE + TURN, rank), bf),
        acc_ga=pltpu.VMEM((rows, cols), f32),
        acc_gp=pltpu.VMEM((rows, cols), f32),
        acc_b=pltpu.VMEM((rows, cols), f32),
        cosine=pltpu.VMEM((n, TURN, rows), f32),
        sine=pltpu.VMEM((n, TURN, rows), f32),
        turn_q=pltpu.VMEM((2, rows, LANES), f32),
        gain_rows=pltpu.VMEM((LANES, rows), f32),
        up_q=pltpu.VMEM((qrank, 2 * heads * LANES), bf),
        up_k=pltpu.VMEM((heads * LANES, rank), bf),
        queries=pltpu.VMEM((heads, rows, LANES), bf),
        lat=pltpu.VMEM((n, 2, rows // 2 + ROPE, rank), bf),
        keys=pltpu.VMEM((2, heads, LANES, 2 * rows), bf),
        values=pltpu.VMEM((2, heads, LANES, 2 * rows), bf),
        attn_acc=pltpu.VMEM((heads, rows, LANES), f32),
        band=pltpu.VMEM((groups, rows, rows + LANES), bf),
        padded=pltpu.VMEM((rows + LANES, pool), bf),
        prow=pltpu.VMEM((2, rows, pool), bf),
        psend=pltpu.VMEM((m // 2 - 1, rows, cols), bf),
        precv=pltpu.VMEM((m // 2 - 1, rows, cols), bf),
        arows=pltpu.VMEM((chunks, m, rows, LANES), bf),
        local_sem=dma((11,)),
        sent=dma,
        tok_sem=dma((4, m - 1)),
        edge_sem=dma((m - 1,)),
        sum_sem=dma,
        fs_sem=dma((m // 2 - 1,)),
        wp_sem=dma((m // 2,)),
        wt_sem=dma((chunks,)),
        wa_sem=dma((m - 2, share)),
        wf_sem=dma((m - 2, share)),
        wz_sem=dma((m - 2, share)),
        ar_sem=dma((chunks, m - 1)),
        pr_sem=dma,
        pp_sem=dma((m // 2 - 1,)),
        halo_sem=dma((2,)),
        main_sem=dma((n - 1,)),
        pair_sem=dma((n,)),
    )
    names = list(inputs) + ["out"] + list(scratch)
    return pl.pallas_call(
        functools.partial(kernel, n, m, names),
        out_shape=pltpu.VMEM((rows, cols), bf),
        in_specs=[pl.BlockSpec(memory_space=pl.ANY)] * len(inputs),
        out_specs=pl.BlockSpec(memory_space=pltpu.VMEM),
        scratch_shapes=list(scratch.values()),
        compiler_params=pltpu.CompilerParams(collective_id=0, has_side_effects=True),
    )(*inputs.values())


def solution(mesh):
    placed = (
        P("sp", "tp"),
        P(),
        P(),
        P(),
        P(None, "tp"),
        P(),
        P(),
        P(),
        P(None, "tp"),
        P(),
        P(),
        P(None, "tp"),
        P("tp", None, None),
        P("tp"),
        P("tp", None),
        P("tp", None),
        P(None, "tp"),
        P(None, "tp"),
    )
    held = functools.partial(body, mesh.shape["sp"], mesh.shape["tp"])
    return jax.shard_map(held, mesh=mesh, in_specs=placed, out_specs=P("sp", "tp"), check_vma=False)
```

```python
import functools
import math
import types

import jax
import numpy as np
import jax.numpy as jnp
from jax import lax
from jax.experimental import pallas as pl
from jax.experimental.pallas import tpu as pltpu
from jax.sharding import PartitionSpec as P

NOPE = 64
ROPE = 32
TURN = ROPE // 2
WIDTH = NOPE + ROPE
VALUE_DIM = 64
POOL_GROUPS = 4
POOL_GROUP = 256
LANES = 128
HALO = 8

eps = 1e-06
theta = 10000.0
f32 = jnp.float32
bf = jnp.bfloat16
MESH = pl.DeviceIdType.MESH
NT = (((1,), (1,)), ((), ()))


def flip(index, offset):
    bit = 1
    while bit <= offset:
        if offset & bit:
            index = index + bit - 2 * bit * ((index // bit) % 2)
        bit *= 2
    return index


def mm(a, b):
    return jnp.dot(a, b, preferred_element_type=f32)


def mm_nt(a, b):
    return lax.dot_general(a, b, NT, preferred_element_type=f32)


def phase(name):
    pass


def kernel(n, m, names, *refs):
    r = types.SimpleNamespace(**dict(zip(names, refs)))
    s = lax.axis_index("sp")
    t = lax.axis_index("tp")
    rows, cols = r.out.shape
    pairs = n // 2
    p = s // 2
    y = s % 2
    half = rows // 2
    across = flip(s, 1)
    twin = flip(t, 1)
    core = t % 2
    other = (s + n + 2 * y - 1) % n
    heads = r.queries.shape[0]
    rank = r.lat.shape[3]
    hc = cols // 2
    tiles = rows // LANES

    nearest = [
        sorted(range(pairs), key=lambda gap: (abs((q + gap) % pairs - q), gap)) for q in range(pairs)
    ]

    def gap_of(i):
        gap = jnp.int32(0)
        for q in range(pairs):
            if isinstance(i, int):
                mine_of = nearest[q][i]
            else:
                mine_of = jnp.int32(0)
                for k in range(1, pairs):
                    mine_of = mine_of + jnp.where(i == k, nearest[q][k], 0)
            gap = gap + jnp.where(p == q, mine_of, 0)
        return gap

    def same_parity(i):
        return ((p + i) % pairs) * 2 + y

    phase("barrier")
    barrier = pltpu.get_barrier_semaphore()
    peers = [(s, flip(t, off)) for off in range(1, m)]
    peers += [(same_parity(i), t) for i in range(1, pairs)]
    peers += [(across, t), (other, t)]
    for peer in peers:
        pl.semaphore_signal(barrier, inc=1, device_id=peer, device_id_type=MESH)

    def columns(block):
        return pl.ds(pl.multiple_of(block * cols, cols), cols)

    fetch = {}

    def take(name, src, dst, slot):
        copy = pltpu.make_async_copy(src, dst, r.local_sem.at[slot])
        copy.start()
        fetch.setdefault(name, []).append(copy)

    def have(*wanted):
        for name in wanted:
            for copy in fetch.pop(name, ()):
                copy.wait()

    take("tokens", r.h_tokens, r.tok.at[0], 0)
    mine = pl.ds(pl.multiple_of(t * cols, cols), cols)
    take("norm_gain", r.h_norm_gain, r.norm_gain, 1)
    take("w_latent_down", r.h_w_latent_down.at[mine, :], r.w_latent_down, 2)
    take("w_rotary", r.h_w_rotary.at[:, mine], r.w_rotary, 3)
    slot = 4
    for name in ("w_query_down", "w_gate_attn", "w_gate_pool", "w_pool_in"):
        for off in range(m):
            rows_of = pl.ds(pl.multiple_of(flip(t, off) * cols, cols), cols)
            place = pl.ds(off * cols, cols)
            source = getattr(r, "h_" + name).at[rows_of, :]
            take(name, source, getattr(r, name).at[place, :], slot)
        slot += 1
    for name in (
        "freqs",
        "w_query_up",
        "w_latent_up",
        "gain_q",
        "gain_k",
        "latent_gain",
        "query_gain",
        "w_pool_mix",
        "pool_scale",
    ):
        take("small", getattr(r, "h_" + name), getattr(r, name), slot)
    depth = r.wa.shape[2]
    for j in range(heads // 2):
        take("wa", r.h_attn_out.at[pl.ds(j * depth, depth), columns(t)], r.wa.at[j, 0], slot + 1)
    for o in range(m // 2):
        take("wp", r.h_pool_out.at[:, columns(flip(t, 2 * o))], r.wp.at[o, 0], slot + 2)

    def ready(off, start, size):
        base = flip(t, off) * cols + start
        raw = r.tok[off, :, start : start + size].astype(f32)
        gain = r.norm_gain[:, pl.ds(pl.multiple_of(base, hc), size)]
        spot = slice(off * cols + start, off * cols + start + size)
        r.scaled[:rows, spot] = (raw * gain).astype(bf)
        return jnp.sum(raw * raw, axis=-1, keepdims=True)

    def ready_edge(off):
        raw = r.edge[off].astype(f32)
        gain = r.norm_gain[:, columns(flip(t, off))]
        r.scaled[rows:, off * cols : (off + 1) * cols] = (raw * gain).astype(bf)
        return jnp.sum(raw * raw, axis=-1, keepdims=True)

    lane = lax.broadcasted_iota(jnp.int32, (1, LANES), 1)
    have("tokens", "norm_gain")
    squares = ready(0, 0, cols)
    have("w_latent_down", "w_rotary")
    part = mm(r.scaled[:rows, :cols], r.w_latent_down[...])
    side = mm_nt(r.scaled[:rows, :cols], r.w_rotary[...])
    side = jnp.concatenate([side, jnp.zeros((rows, LANES - ROPE), f32)], axis=1)
    side = jnp.where(lane == ROPE, squares, side)
    for e in range(2):
        r.sum_own[e, :, :rank] = part[e * half : (e + 1) * half]
        r.sum_own[e, :, rank:] = side[e * half : (e + 1) * half]
    pl.semaphore_wait(barrier, len(peers))

    def remote(src, dst, recv, peer):
        return pltpu.make_async_remote_copy(
            src_ref=src,
            dst_ref=dst,
            send_sem=r.sent,
            recv_sem=recv,
            device_id=peer,
            device_id_type=MESH,
        )

    def push(view, sem, off, least=1, most=m // 2):
        bit = most
        while bit >= least:
            if off == 0 or bit < (off & -off):
                slot = off ^ bit
                remote(view(off), view(slot), sem.at[slot - 1], (s, flip(t, bit))).start()
            bit //= 2

    def arrive(view, sem, off):
        remote(view(0), view(off), sem.at[off - 1], (s, t)).wait_recv()
        push(view, sem, off)

    def drain(view, sem):
        for slot in range(1, m):
            remote(view(0), view(slot), sem.at[slot - 1], (s, t)).wait_send()

    phase("push0")
    sum_copy = remote(r.sum_own.at[1 - core], r.sum_in, r.sum_sem, (s, twin))
    sum_copy.start()
    parts = 4
    width = cols // parts

    def tok_view(c):
        return lambda off: r.tok.at[off, :, pl.ds(c * width, width)]

    push(tok_view(0), r.tok_sem.at[0], 0, 2)
    downward = remote(
        r.tok.at[0, pl.ds(rows - HALO, HALO), :],
        r.edge.at[0, pl.ds(0, HALO), :],
        r.halo_sem.at[0],
        ((s + 1) % n, t),
    )
    upward = remote(
        r.tok.at[0, pl.ds(0, HALO), :],
        r.edge.at[0, pl.ds(HALO, HALO), :],
        r.halo_sem.at[1],
        ((s + n - 1) % n, t),
    )
    downward.start()
    upward.start()
    pair_copies = []
    for o in range(m // 2):
        pair_copies.append(
            remote(
                r.h_pool_out.at[:, columns(flip(twin, 2 * o))],
                r.wp.at[o, 1],
                r.wp_sem.at[o],
                (s, twin),
            )
        )
    for j in range(heads // 2):
        pair_copies.append(
            remote(
                r.h_attn_out.at[pl.ds(j * depth, depth), columns(twin)],
                r.wa.at[j, 1],
                r.wt_sem.at[j],
                (s, twin),
            )
        )
    chunks = heads // 2
    share = chunks // 2

    def shared(half_of):
        return pl.ds(half_of * share, share)

    beside = flip(s, 2)
    level = p % 2
    slab = depth // 2

    def slab_rows(start, which):
        return pl.ds(pl.multiple_of(start + which * slab, slab), slab)

    far_copies = []
    for off in range(2, m):
        for j in range(share):
            piece = y * share + j
            far_copies.append(
                remote(
                    r.h_attn_out.at[slab_rows(piece * depth, level), columns(flip(t, off))],
                    r.wa.at[piece, off, slab_rows(0, level)],
                    r.wa_sem.at[off - 2, j],
                    (s, flip(t, off)),
                )
            )

    def along_line(off, j):
        part = r.wa.at[y * share + j, off, slab_rows(0, level)]
        return remote(part, part, r.wz_sem.at[off - 2, j], (beside, t))

    def over(off, j):
        piece = r.wa.at[y * share + j, off]
        return remote(piece, piece, r.wf_sem.at[off - 2, j], (across, t))

    phase("own")

    def partial(off, w, start, size):
        spot = slice(off * cols + start, off * cols + start + size)
        return mm(r.scaled[:rows, spot], w[spot, :])

    def edge_view(off):
        return r.edge.at[off]

    wides = (
        ("w_query_down", r.acc_q, r.w_query_down),
        ("w_gate_attn", r.acc_ga, r.w_gate_attn),
        ("w_gate_pool", r.acc_gp, r.w_gate_pool),
        ("w_pool_in", r.acc_p, r.w_pool_in),
    )
    first = list(range(max(m // 2, 1)))
    later = list(range(max(m // 2, 1), m))
    for name, acc, w in wides[:1]:
        have(name)
        acc[...] = partial(0, w, 0, cols)

    phase("sum_pair")
    sum_copy.wait_recv()
    total = r.sum_own[core] + r.sum_in[...]
    side = jnp.concatenate([total[:, rank:], jnp.zeros((rank - half, LANES), f32)], axis=0).T
    row = lax.broadcasted_iota(jnp.int32, (TURN, rank), 0)
    levels = side[ROPE : ROPE + 1]
    coarse = levels.astype(bf).astype(f32)
    tail = jnp.where(row == 0, coarse, jnp.where(row == 1, levels - coarse, 0.0))
    r.sum_main[...] = total[:, :rank]
    r.sum_side[...] = side[: ROPE + 8]
    r.far_out[:half, :] = total[:, :rank].astype(bf)
    r.far_out[half : half + ROPE, :] = side[:ROPE].astype(bf)
    r.far_out[half + ROPE :, :] = tail.astype(bf)
    far_sums = []
    for off in range(2, m, 2):
        far_sums.append(
            remote(
                r.far_out,
                r.far_in.at[off // 2 - 1],
                r.fs_sem.at[off // 2 - 1],
                (s, flip(t, off)),
            )
        )
        far_sums[-1].start()
    for c in range(1, parts - 1):
        push(tok_view(c), r.tok_sem.at[c], 0, 2)
    for c in range(parts):
        push(tok_view(c), r.tok_sem.at[c], 0, 1, 1)

    phase("own2")
    for name, acc, w in wides[1:]:
        have(name)
        acc[...] = partial(0, w, 0, cols)
    phase("edge")
    downward.wait_recv()
    upward.wait_recv()
    push(edge_view, r.edge_sem, 0)
    push(tok_view(parts - 1), r.tok_sem.at[parts - 1], 0, 2)
    for copy in pair_copies:
        copy.start()
    phase("own3")
    squares_edge = ready_edge(0)
    for off in first[1:]:
        for c in range(parts):
            arrive(tok_view(c), r.tok_sem.at[c], off)
        squares += ready(off, 0, cols)
        for name, acc, w in wides:
            acc[...] += partial(off, w, 0, cols)
    for off in first[1:]:
        arrive(edge_view, r.edge_sem, off)
        squares_edge += ready_edge(off)
    span = len(first) * cols
    r.acc_e[...] = mm(r.scaled[rows:, :span], r.w_pool_in[:span, :])

    have("small")

    def rms(values, gain, width):
        mean = jnp.sum(values * values, axis=-1, keepdims=True) / width
        return values * lax.rsqrt(mean + eps) * gain

    phase("sum_far")
    main = r.sum_main[...]
    side = r.sum_side[:ROPE, :]
    levels = r.sum_side[ROPE : ROPE + 1, :]
    for i, copy in enumerate(far_sums):
        copy.wait_recv()
        main += r.far_in[i, :half, :].astype(f32)
        side += r.far_in[i, half : half + ROPE, :].astype(f32)
        tail = r.far_in[i, half + ROPE :, :].astype(f32)
        levels += tail[:1] + tail[1:2]
    level_row = lax.rsqrt(levels / (cols * m) + eps)
    level_column = jnp.broadcast_to(level_row, (LANES, rank)).T[:half, :1]
    latent = (main * level_column).astype(bf).astype(f32)
    r.lat[0, core, :half, :] = rms(latent, r.latent_gain[...], rank).astype(bf)
    r.lat[0, core, half:, :] = (side * level_row).astype(bf)

    near_copy = remote(
        r.lat.at[0, core], r.lat.at[1, core], r.main_sem.at[0], (across, t)
    )
    near_copy.start()

    def send(i):
        gap = (pairs - gap_of(i)) % pairs
        remote(
            r.lat.at[0, core],
            r.lat.at[2 * gap, core],
            r.main_sem.at[2 * gap - 1],
            (same_parity(pairs - gap), t),
        ).start()

    inner = (p > 0) & (p < pairs - 1)
    head = p == 0
    tail_end = p == pairs - 1

    def only(condition, act, i):
        if i < pairs:

            @pl.when(condition)
            def _():
                act(i)

    send(1)
    only(inner, send, 2)

    def main_wait(k):
        remote(
            r.lat.at[0, core], r.lat.at[k, core], r.main_sem.at[k - 1], (s, t)
        ).wait_recv()

    def to_across(k):
        return remote(
            r.lat.at[k, core], r.lat.at[k + 1, core], r.main_sem.at[k], (across, t)
        )

    def to_twin(k):
        return remote(
            r.lat.at[k, core], r.lat.at[k, core], r.pair_sem.at[k], (s, twin)
        )

    def twin_wait(k):
        remote(
            r.lat.at[k, core], r.lat.at[k, 1 - core], r.pair_sem.at[k], (s, twin)
        ).wait_recv()

    to_twin(0).start()

    phase("tables")
    freqs = jnp.concatenate([r.freqs[...]] * tiles, axis=1)
    along = lax.broadcasted_iota(jnp.int32, (ROPE, rows), 1)

    def table(k, carry):
        source = ((p + k // 2) % pairs) * 2 + (y + k) % 2
        angles = (source * rows + along[:TURN]).astype(f32) * freqs
        r.cosine[k] = jnp.cos(angles)
        r.sine[k] = jnp.sin(angles)
        return carry

    lax.fori_loop(0, n, table, 0)

    low = lane < NOPE
    spare = jnp.zeros((1, LANES - WIDTH), f32)
    turning = (lane >= NOPE) & (lane < WIDTH)

    def partner(values):
        swapped = jnp.where(
            lane < NOPE + TURN,
            pltpu.roll(values, LANES - TURN, 1),
            pltpu.roll(values, TURN, 1),
        )
        return jnp.where(turning, swapped, 0.0)

    gain_q = jnp.concatenate([r.gain_q[...], spare], axis=1)
    gain_q = gain_q * (WIDTH**-0.5 * math.log2(math.e))
    gain_q = jnp.broadcast_to(gain_q, (8, LANES))
    gain_p = partner(gain_q)
    side = jnp.zeros((LANES - WIDTH, rows), f32)
    cosine = jnp.concatenate([jnp.ones((NOPE, rows), f32), r.cosine[0], r.cosine[0], side], axis=0)
    sine = jnp.concatenate([jnp.zeros((NOPE, rows), f32), -r.sine[0], r.sine[0], side], axis=0)
    r.turn_q[0] = cosine.T * gain_q[:1]
    r.turn_q[1] = sine.T * gain_p[:1]
    gain_k = jnp.concatenate([r.gain_k[...], spare], axis=1)
    gain_k = jnp.broadcast_to(gain_k, (LANES, LANES)).T
    r.gain_rows[...] = jnp.concatenate([gain_k] * tiles, axis=1)

    for h in range(heads):
        up = r.w_query_up[:, h * WIDTH : (h + 1) * WIDTH].astype(f32)
        up = jnp.concatenate([up, jnp.zeros((up.shape[0], LANES - WIDTH), f32)], axis=1)
        r.up_q[:, h * LANES : (h + 1) * LANES] = up.astype(bf)
        r.up_q[:, (heads + h) * LANES : (heads + h + 1) * LANES] = partner(up).astype(bf)
    r.up_k[...] = r.w_latent_up[...].astype(f32).T.astype(bf)
    for e in range(2):
        for h in range(heads):
            r.keys[e, h, WIDTH:, :] = jnp.zeros((LANES - WIDTH, 2 * rows), bf)
            row = lax.broadcasted_iota(jnp.int32, (LANES - VALUE_DIM, 2 * rows), 0)
            r.values[e, h, VALUE_DIM:, :] = jnp.where(row == 0, 1.0, 0.0).astype(bf)
    r.attn_acc[...] = jnp.zeros_like(r.attn_acc)
    groups = r.w_pool_mix.shape[0]
    column = lax.broadcasted_iota(jnp.int32, (rows, rows + LANES), 1)
    before = (column >= rows) & (column < rows + HALO)
    column = jnp.where(before, column - rows - HALO, jnp.where(column < rows, column, column - HALO))
    apart = column - lax.broadcasted_iota(jnp.int32, (rows, rows + LANES), 0)
    place = s * rows + column
    exists = (place >= 0) & (place < rows * n)

    def reach_of(j):
        group = t * groups + j
        reach = jnp.int32(0)
        for i in range(POOL_GROUPS):
            reach = reach + jnp.where(group == i, 2**i, 0)
        return reach

    for j in range(groups):
        reach = reach_of(j)
        inside = exists & (apart >= -reach) & (apart <= reach - 1)
        r.band[j] = jnp.where(inside, 1.0, 0.0).astype(bf)
    pool = r.padded.shape[1]
    r.padded[pl.ds(rows + 2 * HALO, LANES - 2 * HALO), :] = jnp.zeros(
        (LANES - 2 * HALO, pool), bf
    )

    def gather_tokens(h):
        total = 0.0
        for c in range(h * parts // 2, (h + 1) * parts // 2):
            for off in later:
                arrive(tok_view(c), r.tok_sem.at[c], off)
            if c == 0:
                only(head, send, 2)
                only(jnp.logical_not(head), send, 3)
            if c == parts // 2:
                only(head, send, 3)
                only(tail_end, send, 2)
                for i in range(4, pairs):
                    send(i)
                for copy in far_copies:
                    copy.start()
                only(inner, forward, 2)
        for off in later:
            total += ready(off, h * hc, hc)
        return total

    def prepare(k, slot, e):
        latent = jnp.concatenate([r.lat[k, 0, :half, :], r.lat[k, 1, :half, :]], axis=0)

        def turns(part):
            got = r.lat[k, part, half:, :].astype(f32)
            return jnp.concatenate([got, jnp.zeros((ROPE, rows - rank), f32)], axis=1)

        whole = jnp.where(along < half, turns(0), pltpu.roll(turns(1), half, 1))
        x1 = whole[:TURN]
        x2 = whole[TURN:]
        shared_sum = jnp.sum(x1 * x1 + x2 * x2, axis=0, keepdims=True)
        x1 = x1 * r.gain_rows[NOPE : NOPE + TURN, :]
        x2 = x2 * r.gain_rows[NOPE + TURN : WIDTH, :]
        cosine = r.cosine[k]
        sine = r.sine[k]
        turn1 = x1 * cosine - x2 * sine
        turn2 = x1 * sine + x2 * cosine
        both = mm_nt(r.up_k[...], latent)
        spot = slice(e * rows, (e + 1) * rows)
        for h in range(heads):
            plain = both[h * LANES : h * LANES + NOPE].astype(bf).astype(f32)
            value = both[h * LANES + NOPE : (h + 1) * LANES].astype(bf)
            total = jnp.sum(plain * plain, axis=0, keepdims=True)
            level = lax.rsqrt((total + shared_sum) / WIDTH + eps)
            r.keys[slot, h, :NOPE, spot] = (plain * r.gain_rows[:NOPE, :] * level).astype(bf)
            r.keys[slot, h, NOPE : NOPE + TURN, spot] = (turn1 * level).astype(bf)
            r.keys[slot, h, NOPE + TURN : WIDTH, spot] = (turn2 * level).astype(bf)
            r.values[slot, h, :VALUE_DIM, spot] = value

    def attend(slot, h):
        scores = mm(r.queries[h], r.keys[slot, h])
        weighted = mm_nt(jnp.exp2(scores).astype(bf), r.values[slot, h])
        r.attn_acc[h] += weighted

    def forward(i):
        ahead = 2 * gap_of(i)
        main_wait(ahead)
        to_across(ahead).start()
        to_twin(ahead).start()

    def gather(i):
        now = 2 * gap_of(i)
        main_wait(now + 1)
        to_twin(now + 1).start()

    phase("later0")
    squares += gather_tokens(0)
    for name, acc, w in wides:
        total = acc[...]
        for off in later:
            total += partial(off, w, 0, hc)
        acc[...] = total

    phase("prep0")
    twin_wait(0)
    prepare(0, 0, 0)
    phase("across0")
    gather(0)
    phase("ahead1")
    forward(1)
    phase("later1")
    for off in later:
        arrive(edge_view, r.edge_sem, off)
        squares_edge += ready_edge(off)
    r.acc_e[...] += mm(r.scaled[rows:, span:], r.w_pool_in[span:, :])
    squares += gather_tokens(1)
    scale = lax.rsqrt(squares / (cols * m) + eps)

    def finish(acc, w):
        total = acc[...]
        for off in later:
            total += partial(off, w, hc, hc)
        return total

    phase("head2")
    only(head, forward, 2)
    phase("pool_input")
    scale_edge = lax.rsqrt(squares_edge / (cols * m) + eps)
    r.padded[:rows, :] = (finish(r.acc_p, r.w_pool_in) * scale).astype(bf)
    r.padded[rows : rows + 2 * HALO, :] = (r.acc_e[...] * scale_edge).astype(bf)
    phase("pool")
    position = s * rows + lax.broadcasted_iota(jnp.int32, (rows, 1), 0)
    for j in range(groups):
        reach = reach_of(j)
        part = slice(j * POOL_GROUP, (j + 1) * POOL_GROUP)
        total = mm(r.band[j], r.padded[:, part])
        start = jnp.maximum(position - reach, 0)
        stop = jnp.minimum(position + reach, rows * n)
        count = (stop - start).astype(f32)
        own = r.padded[:rows, part].astype(f32)
        mixed = (total / count - own).astype(bf)
        r.prow[0, :, part] = (mm(mixed, r.w_pool_mix[j]) * r.pool_scale[:, part]).astype(bf)
    prow_copy = remote(r.prow.at[0], r.prow.at[1], r.pr_sem, (s, twin))
    prow_copy.start()
    phase("query")
    query_latent = (finish(r.acc_q, r.w_query_down) * scale).astype(bf).astype(f32)
    query_normed = rms(query_latent, r.query_gain[...], query_latent.shape[1]).astype(bf)
    query_raw = mm(query_normed, r.up_q[...])
    for h in range(heads):
        raw = query_raw[:, h * LANES : (h + 1) * LANES].astype(bf).astype(f32)
        swapped = query_raw[:, (heads + h) * LANES : (heads + h + 1) * LANES].astype(bf).astype(f32)
        mean = jnp.sum(raw * raw, axis=-1, keepdims=True) / WIDTH
        turned = raw * r.turn_q[0] + swapped * r.turn_q[1]
        r.queries[h] = (turned * lax.rsqrt(mean + eps)).astype(bf)

    phase("ahead2")
    only(tail_end, forward, 2)
    only(jnp.logical_not(tail_end), forward, 3)
    def relay_line():
        for off in range(2, m):
            for j in range(share):
                far_copies[(off - 2) * share + j].wait_recv()
                along_line(off, j).start()

    phase("across1")
    gather(1)
    phase("pool_out")
    prow_copy.wait_recv()
    have("wp")
    for o in range(m // 2):
        pair_copies[o].wait_recv()
    part_copies = []
    pool_rows = jnp.concatenate([r.prow[0], r.prow[1]], axis=1)
    for o in range(m // 2 - 1, -1, -1):
        weights = jnp.concatenate([r.wp[o, 0], r.wp[o, 1]], axis=0)
        branch = mm(pool_rows, weights)
        if o:
            r.psend[o - 1] = branch.astype(bf)
            copy = remote(
                r.psend.at[o - 1],
                r.precv.at[o - 1],
                r.pp_sem.at[o - 1],
                (s, flip(t, 2 * o)),
            )
            copy.start()
            part_copies.append(copy)
        else:
            r.acc_b[...] = branch

    phase("relay_line")
    relay_line()
    phase("pair0")
    twin_wait(1)
    prepare(1, 0, 1)
    for h in range(heads):
        attend(0, h)
    phase("ahead3")
    only(tail_end, forward, 3)
    def relay():
        for off in range(2, m):
            for j in range(share):
                remote(
                    r.wa.at[y * share + j, off, slab_rows(0, level)],
                    r.wa.at[y * share + j, off, slab_rows(0, 1 - level)],
                    r.wz_sem.at[off - 2, j],
                    (beside, t),
                ).wait_recv()
                over(off, j).start()

    phase("steps")

    def step(i, carry):
        now = 2 * gap_of(i)

        @pl.when(i + 3 < pairs)
        def _():
            forward(i + 3)

        twin_wait(now)
        twin_wait(now + 1)
        prepare(now, i % 2, 0)
        prepare(now + 1, i % 2, 1)
        for h in range(chunks):
            attend(i % 2, h)
        gather(i + 1)

        @pl.when(i == pairs - 2)
        def _():
            relay()

        for h in range(chunks, heads):
            attend(i % 2, h)
        return carry

    lax.fori_loop(1, pairs - 1, step, 0)

    phase("last_wait")
    i = pairs - 1
    now = 2 * gap_of(i)
    twin_wait(now)
    twin_wait(now + 1)
    phase("last_attend")
    prepare(now, i % 2, 0)
    prepare(now + 1, i % 2, 1)

    def rows_view(j):
        return lambda off: r.arows.at[j, off]

    order = [y * share + j for j in range(share)] + [(1 - y) * share + j for j in range(share)]
    for j, chunk in enumerate(order):
        for h in (2 * chunk, 2 * chunk + 1):
            attend(i % 2, h)
        even = r.attn_acc[2 * chunk]
        odd = r.attn_acc[2 * chunk + 1]
        even = even / even[:, VALUE_DIM : VALUE_DIM + 1]
        odd = odd / odd[:, VALUE_DIM : VALUE_DIM + 1]
        r.arows[j, 0] = jnp.where(low, even, pltpu.roll(odd, VALUE_DIM, 1)).astype(bf)
        push(rows_view(j), r.ar_sem.at[j], 0)

    phase("gates")
    r.acc_ga[...] = lax.logistic(finish(r.acc_ga, r.w_gate_attn) * scale)
    r.acc_gp[...] = lax.logistic(finish(r.acc_gp, r.w_gate_pool) * scale)

    phase("pool_sum")
    branch = r.acc_b[...]
    for copy in part_copies:
        copy.wait_recv()
    for o in range(1, m // 2):
        branch += r.precv[o - 1].astype(f32)
    r.acc_gp[...] *= branch

    phase("w_wait")
    have("wa")
    for j in range(chunks):
        pair_copies[m // 2 + j].wait_recv()
    total = None
    for j in range(chunks):
        phase("rows%d" % j)
        for off in range(1, m - 1):
            arrive(rows_view(j), r.ar_sem.at[j], off)
        if j == share:
            for off in range(2, m):
                for k in range(share):
                    remote(
                        r.wa.at[0, off],
                        r.wa.at[(1 - y) * share + k, off],
                        r.wf_sem.at[off - 2, k],
                        (across, t),
                    ).wait_recv()
        left = jnp.concatenate([r.arows[j, off] for off in range(m - 1)], axis=1)
        branch = mm(left, r.wa[order[j], : m - 1].reshape((m - 1) * depth, cols))
        total = branch if total is None else total + branch
        arrive(rows_view(j), r.ar_sem.at[j], m - 1)
        phase("out%d" % j)
        total += mm(r.arows[j, m - 1], r.wa[order[j], m - 1])
    r.out[...] = (r.acc_ga[...] * total + r.acc_gp[...]).astype(bf)

    phase("drain")
    for c in range(parts):
        drain(tok_view(c), r.tok_sem.at[c])
    drain(edge_view, r.edge_sem)
    for j in range(chunks):
        drain(rows_view(j), r.ar_sem.at[j])
    for copy in pair_copies + far_copies + part_copies + far_sums + [sum_copy, prow_copy, downward, upward]:
        copy.wait_send()
    for off in range(2, m):
        for j in range(share):
            over(off, j).wait_send()
            along_line(off, j).wait_send()
    for i in range(pairs):
        remote(r.lat.at[0, core], r.lat.at[0, core], r.main_sem.at[0], (s, t)).wait_send()
    for k in range(n):
        to_twin(k).wait_send()
        if k and k % 2 == 0:
            to_across(k).wait_send()
    phase(None)


def body(
    n,
    m,
    tokens,
    norm_gain,
    w_query_down,
    query_gain,
    w_query_up,
    w_latent_down,
    latent_gain,
    w_rotary_key,
    w_latent_up,
    query_head_gain,
    key_head_gain,
    w_pool_in,
    w_pool_mix,
    pool_scale,
    w_attn_out,
    w_pool_out,
    w_gate_attn,
    w_gate_pool,
):
    rows, cols = tokens.shape
    heads = w_query_up.shape[1] // WIDTH
    rank = w_latent_down.shape[1]
    qrank = w_query_down.shape[1]
    pool = w_pool_in.shape[1]
    groups = w_pool_mix.shape[0]
    chunks = heads // 2
    share = chunks // 2
    depth = w_attn_out.shape[0] // chunks
    freqs = np.repeat(theta ** (-np.arange(TURN) / TURN)[:, None], LANES, axis=1)
    dma = pltpu.SemaphoreType.DMA
    inputs = {
        "h_tokens": tokens,
        "h_norm_gain": norm_gain[None, :],
        "h_w_query_down": w_query_down,
        "h_query_gain": query_gain[None, :],
        "h_w_query_up": w_query_up,
        "h_w_latent_down": w_latent_down,
        "h_latent_gain": latent_gain[None, :],
        "h_w_rotary": w_rotary_key.T,
        "h_w_latent_up": w_latent_up,
        "h_gain_q": query_head_gain[None, :],
        "h_gain_k": key_head_gain[None, :],
        "h_w_pool_in": w_pool_in,
        "h_w_pool_mix": w_pool_mix,
        "h_pool_scale": pool_scale[None, :],
        "h_attn_out": w_attn_out,
        "h_pool_out": w_pool_out,
        "h_w_gate_attn": w_gate_attn,
        "h_w_gate_pool": w_gate_pool,
        "h_freqs": jnp.asarray(freqs, f32),
    }
    scratch = {}
    for name, value in inputs.items():
        if name not in ("h_tokens", "h_attn_out", "h_pool_out"):
            scratch[name[2:]] = pltpu.VMEM(value.shape, value.dtype)
    scratch["w_latent_down"] = pltpu.VMEM((cols, rank), bf)
    scratch["w_rotary"] = pltpu.VMEM((ROPE, cols), bf)
    scratch.update(
        tok=pltpu.VMEM((m, rows, cols), bf),
        scaled=pltpu.VMEM((rows + 2 * HALO, m * cols), bf),
        edge=pltpu.VMEM((m, 2 * HALO, cols), bf),
        acc_p=pltpu.VMEM((rows, pool), f32),
        acc_e=pltpu.VMEM((2 * HALO, pool), f32),
        wa=pltpu.VMEM((chunks, m, depth, cols), bf),
        wp=pltpu.VMEM((m // 2, 2, pool, cols), bf),
        acc_q=pltpu.VMEM((rows, qrank), f32),
        sum_own=pltpu.VMEM((2, rows // 2, rank + LANES), f32),
        sum_in=pltpu.VMEM((rows // 2, rank + LANES), f32),
        sum_main=pltpu.VMEM((rows // 2, rank), f32),
        sum_side=pltpu.VMEM((ROPE + 8, rank), f32),
        far_out=pltpu.VMEM((rows // 2 + ROPE + TURN, rank), bf),
        far_in=pltpu.VMEM((m // 2 - 1, rows // 2 + ROPE + TURN, rank), bf),
        acc_ga=pltpu.VMEM((rows, cols), f32),
        acc_gp=pltpu.VMEM((rows, cols), f32),
        acc_b=pltpu.VMEM((rows, cols), f32),
        cosine=pltpu.VMEM((n, TURN, rows), f32),
        sine=pltpu.VMEM((n, TURN, rows), f32),
        turn_q=pltpu.VMEM((2, rows, LANES), f32),
        gain_rows=pltpu.VMEM((LANES, rows), f32),
        up_q=pltpu.VMEM((qrank, 2 * heads * LANES), bf),
        up_k=pltpu.VMEM((heads * LANES, rank), bf),
        queries=pltpu.VMEM((heads, rows, LANES), bf),
        lat=pltpu.VMEM((n, 2, rows // 2 + ROPE, rank), bf),
        keys=pltpu.VMEM((2, heads, LANES, 2 * rows), bf),
        values=pltpu.VMEM((2, heads, LANES, 2 * rows), bf),
        attn_acc=pltpu.VMEM((heads, rows, LANES), f32),
        band=pltpu.VMEM((groups, rows, rows + LANES), bf),
        padded=pltpu.VMEM((rows + LANES, pool), bf),
        prow=pltpu.VMEM((2, rows, pool), bf),
        psend=pltpu.VMEM((m // 2 - 1, rows, cols), bf),
        precv=pltpu.VMEM((m // 2 - 1, rows, cols), bf),
        arows=pltpu.VMEM((chunks, m, rows, LANES), bf),
        local_sem=dma((11,)),
        sent=dma,
        tok_sem=dma((4, m - 1)),
        edge_sem=dma((m - 1,)),
        sum_sem=dma,
        fs_sem=dma((m // 2 - 1,)),
        wp_sem=dma((m // 2,)),
        wt_sem=dma((chunks,)),
        wa_sem=dma((m - 2, share)),
        wf_sem=dma((m - 2, share)),
        wz_sem=dma((m - 2, share)),
        ar_sem=dma((chunks, m - 1)),
        pr_sem=dma,
        pp_sem=dma((m // 2 - 1,)),
        halo_sem=dma((2,)),
        main_sem=dma((n - 1,)),
        pair_sem=dma((n,)),
    )
    names = list(inputs) + ["out"] + list(scratch)
    return pl.pallas_call(
        functools.partial(kernel, n, m, names),
        out_shape=pltpu.VMEM((rows, cols), bf),
        in_specs=[pl.BlockSpec(memory_space=pl.ANY)] * len(inputs),
        out_specs=pl.BlockSpec(memory_space=pltpu.VMEM),
        scratch_shapes=list(scratch.values()),
        compiler_params=pltpu.CompilerParams(collective_id=0, has_side_effects=True),
    )(*inputs.values())


def solution(mesh):
    placed = (
        P("sp", "tp"),
        P(),
        P(),
        P(),
        P(None, "tp"),
        P(),
        P(),
        P(),
        P(None, "tp"),
        P(),
        P(),
        P(None, "tp"),
        P("tp", None, None),
        P("tp"),
        P("tp", None),
        P("tp", None),
        P(None, "tp"),
        P(None, "tp"),
    )
    held = functools.partial(body, mesh.shape["sp"], mesh.shape["tp"])
    return jax.shard_map(held, mesh=mesh, in_specs=placed, out_specs=P("sp", "tp"), check_vma=False)
```
